128 devices in a mesh: dp: 4 (over x), kv: 16 (over z, y), tp: 2 (over core).
Axes of the slice: x: 4, y: 4, z: 4, core: 2. Of those that a mesh axis runs over, the one named last changes fastest.
Arguments:
- tokens: bfloat16 [32, 2048], P('dp', ('kv', 'tp')), may hold values from -30 to 30
- attention_gain: bfloat16 [2048], P(('kv', 'tp')), may hold values from 0.099609375 to 1.8984375
- query_one: bfloat16 [2048, 512], P('kv', 'tp'), may hold values from -0.125 to 0.125
- query_two: bfloat16 [2048, 512], P('kv', 'tp'), may hold values from -0.125 to 0.125
- key_one: bfloat16 [2048, 512], P('kv', 'tp'), may hold values from -2 to 2
- key_two: bfloat16 [2048, 512], P('kv', 'tp'), may hold values from -2 to 2
- value_weight: bfloat16 [2048, 1024], P('kv', 'tp'), may hold values from -0.125 to 0.125
- head_second_weight: float32 [8], P('tp'), may hold values from 0.3 to 0.8
- head_gain: float32 [128], replicated, may hold values from 0.1 to 1.9
- out_weight: bfloat16 [1024, 2048], P('tp', 'kv'), may hold values from -0.375 to 0.375
- mixer_gain: bfloat16 [2048], P(('kv', 'tp')), may hold values from 0.099609375 to 1.8984375
- gate_weight: bfloat16 [2048, 5632], P('kv', 'tp'), may hold values from -0.125 to 0.125
- up_weight: bfloat16 [2048, 5632], P('kv', 'tp'), may hold values from -0.125 to 0.125
- down_weight: bfloat16 [5632, 2048], P('tp', 'kv'), may hold values from -0.15625 to 0.15625
- key_cache: bfloat16 [32, 16384, 8, 128], P('dp', 'kv', 'tp'), may hold values from -240 to 240
- value_cache: bfloat16 [32, 16384, 8, 128], P('dp', 'kv', 'tp'), may hold values from -6 to 6
Outputs:
- layer_out: bfloat16 [32, 2048], P('dp', ('kv', 'tp'))
The draws below stay inside these ranges and needn't reach their ends.
All inputs are finite; a program needn't handle non-finite values.
Results may differ from the reference program's by a relative error of at most 0.02.
Values may be sent and summed in bfloat16 or wider, within the bound.
A program may use at most 64 MiB of HBM per device.

```python
import jax
import jax.numpy as jnp
from jax import lax

D = 2048
HEADS = 8
DH = 64
FF = 5632
POS_DEV = 1024
BATCH = 32
CACHE = 16384
N_TP = 2


def draw_tokens(key, part):
    columns = jnp.arange(D, dtype=jnp.float32)
    rising = jnp.exp(jnp.log(4.0) * columns / (D - 1))
    rough = jax.random.uniform(jax.random.fold_in(key, 11), (D,), jnp.float32, 0.5, 1.5)
    values = jnp.clip(jax.random.normal(jax.random.fold_in(key, 12), (BATCH, D), jnp.float32), -4.0, 4.0)
    return jnp.clip(values * rising * rough, -30.0, 30.0).astype(jnp.bfloat16)


def draw_key_cache(key, part):
    shape = (BATCH, CACHE, HEADS, 2 * DH)
    base = jnp.clip(jax.random.normal(jax.random.fold_in(key, 21), shape, jnp.float32) * 1.75, -10.5, 10.5)
    block_scale = jnp.exp(jax.random.uniform(jax.random.fold_in(key, 25), (BATCH, CACHE // POS_DEV, HEADS), jnp.float32, jnp.log(0.3), jnp.log(3.0)))
    base = base * jnp.repeat(block_scale, POS_DEV, axis=1)[..., None]
    row_boost = jnp.exp(jax.random.uniform(jax.random.fold_in(key, 24), (BATCH, 1, 1, 1), jnp.float32, jnp.log(30.0), jnp.log(60.0)))
    heavy_rows = (jnp.arange(BATCH) % 4 == 0)[:, None, None, None]
    base = jnp.where(heavy_rows, base * row_boost, base)
    return jnp.clip(base, -240.0, 240.0).astype(jnp.bfloat16)


def shard_levels(rng, shape, cuts, least, largest):
    def one(dim, parts):
        heights = jax.random.uniform(jax.random.fold_in(jax.random.fold_in(rng, 6), dim), (parts,), jnp.float32, least / len(cuts), largest / len(cuts))
        return jnp.repeat(jnp.exp(heights), shape[dim] // parts).reshape((-1,) + (1,) * (len(shape) - dim - 1))

    loudness = one(*cuts[0])
    for cut in cuts[1:]:
        loudness = loudness * one(*cut)
    return loudness


def gaussian(stream_key, shape, spread, most, shards=(), kind=jnp.bfloat16):
    values = spread * jax.random.normal(stream_key, shape, jnp.float32)
    if shards:
        values = values * shard_levels(stream_key, shape, shards, -0.22, 0.18)
    return jnp.clip(values, -most, most).astype(kind)


def setup_inputs(seed: int = 0) -> dict:
    seeds = jax.random.split(jax.random.key(seed), 17)
    return {
        "tokens": draw_tokens(jax.random.fold_in(seeds[16], 71), 0),
        "attention_gain": jnp.clip(1.0 + 0.18 * jax.random.normal(seeds[1], (D,), jnp.float32), 0.099609375, 1.8984375).astype(jnp.bfloat16),
        "query_one": gaussian(seeds[2], (D, HEADS * DH), D ** -0.5, 0.125, ((0, 16), (1, 2))),
        "query_two": gaussian(seeds[3], (D, HEADS * DH), D ** -0.5, 0.125, ((0, 16), (1, 2))),
        "key_one": gaussian(seeds[4], (D, HEADS * DH), (D // 256) ** -0.5, 2.0, ((0, 16), (1, 2))),
        "key_two": gaussian(seeds[5], (D, HEADS * DH), (D // 256) ** -0.5, 2.0, ((0, 16), (1, 2))),
        "value_weight": gaussian(seeds[6], (D, HEADS * 2 * DH), D ** -0.5, 0.125, ((0, 16), (1, 2))),
        "head_second_weight": jnp.clip(0.3 + 0.5 * jax.random.uniform(seeds[7], (HEADS,), jnp.float32) ** shard_levels(seeds[7], (HEADS,), ((0, 2),), -0.2, 0.2), 0.3, 0.8),
        "head_gain": jnp.clip(1.0 + 0.18 * jax.random.normal(seeds[8], (2 * DH,), jnp.float32), 0.1, 1.9),
        "out_weight": gaussian(seeds[9], (HEADS * 2 * DH, D), (HEADS * DH // 2) ** -0.5, 0.375, ((0, 2), (1, 16))),
        "mixer_gain": jnp.clip(1.0 + 0.18 * jax.random.normal(seeds[10], (D,), jnp.float32), 0.099609375, 1.8984375).astype(jnp.bfloat16),
        "gate_weight": gaussian(seeds[11], (D, FF), D ** -0.5, 0.125, ((0, 16), (1, 2))),
        "up_weight": gaussian(seeds[12], (D, FF), D ** -0.5, 0.125, ((0, 16), (1, 2))),
        "down_weight": gaussian(seeds[13], (FF, D), (FF // 4) ** -0.5, 0.15625, ((0, 2), (1, 16))),
        "key_cache": draw_key_cache(jax.random.fold_in(seeds[16], 71), 0),
        "value_cache": gaussian(seeds[15], (BATCH, CACHE, HEADS, 2 * DH), 1.0, 6.0, ((0, 4), (1, 16), (2, 2))),
    }


NORM_EPSILON = 1e-06
HEAD_EPSILON = 1e-05
HEAD_SCALE = 0.8
ROTARY_BASE = 10000.0

def rotate(vectors, position):
    half_width = vectors.shape[-1] // 2
    frequency = 1.0 / ROTARY_BASE ** (jnp.arange(half_width, dtype=jnp.float32) / half_width)
    angles = position * frequency
    cosine = jnp.cos(angles)
    sine_value = jnp.sin(angles)
    lead_half = vectors[..., :half_width]
    tail_half = vectors[..., half_width:]
    return jnp.concatenate([lead_half * cosine - tail_half * sine_value, tail_half * cosine + lead_half * sine_value], axis=-1)

def rounded(values):
    return lax.optimization_barrier(values.astype(jnp.bfloat16)).astype(jnp.float32)

def grouped_product(left, right, groups):
    group_width = left.shape[1] // groups
    result = jnp.zeros((left.shape[0], right.shape[1]), jnp.float32)
    for group_index in range(groups):
        group_term = jnp.dot(left[:, group_index * group_width:(group_index + 1) * group_width], right[group_index * group_width:(group_index + 1) * group_width], preferred_element_type=jnp.float32)
        result = result + rounded(group_term)
    return result

def reference(tokens, attention_gain, query_one, query_two, key_one, key_two, value_weight, head_second_weight, head_gain, out_weight, mixer_gain, gate_weight, up_weight, down_weight, key_cache, value_cache):
    position = jnp.float32(CACHE)
    score_scale = DH ** (-0.5)
    token_values = tokens.astype(jnp.float32)
    row_ratio = lax.rsqrt(lax.optimization_barrier(jnp.mean(token_values * token_values, axis=1, keepdims=True)) + NORM_EPSILON)
    scaled = (token_values * attention_gain.astype(jnp.float32)).astype(jnp.bfloat16)

    def project(weight_matrix):
        return jnp.dot(scaled, weight_matrix, preferred_element_type=jnp.float32) * row_ratio

    def paired(lead_matrix, tail_matrix):
        both = jnp.stack([project(lead_matrix).reshape(BATCH, HEADS, DH), project(tail_matrix).reshape(BATCH, HEADS, DH)], axis=2)
        return rotate(both, position).astype(jnp.bfloat16)
    queries = paired(query_one, query_two)
    new_keys = paired(key_one, key_two)
    new_values = project(value_weight).astype(jnp.bfloat16).reshape(BATCH, HEADS, 2 * DH)

    def one_sequence(operands):
        query, new_key, new_value, cached_keys, cached_values = operands
        query_entries = query.astype(jnp.float32)
        key_entries = cached_keys.astype(jnp.float32).reshape(CACHE, HEADS, 2, DH)
        logit_scores = jnp.einsum('tvs,ntvs->tvn', query_entries, key_entries) * score_scale
        own_score = lax.optimization_barrier(jnp.sum(query_entries * new_key.astype(jnp.float32), axis=-1)) * score_scale
        peak_score = jnp.maximum(lax.optimization_barrier(jnp.max(logit_scores, axis=-1)), own_score)
        exponent = jnp.exp(logit_scores - peak_score[..., None])
        own_weight = jnp.exp(own_score - peak_score)
        weight_sum = lax.optimization_barrier(jnp.sum(exponent, axis=-1)) + own_weight
        weighted = jnp.einsum('hmp,phe->hme', rounded(exponent), cached_values.astype(jnp.float32))
        weighted = weighted + own_weight[..., None] * new_value.astype(jnp.float32)[:, None, :]
        averaged = weighted / weight_sum[..., None]
        difference = averaged[:, 0] - head_second_weight[:, None] * averaged[:, 1]
        inverse_norm = lax.rsqrt(lax.optimization_barrier(jnp.mean(difference * difference, axis=-1, keepdims=True)) + HEAD_EPSILON)
        return (difference * inverse_norm * head_gain[None, :] * HEAD_SCALE).astype(jnp.bfloat16)
    attended = lax.map(one_sequence, (queries, new_keys, new_values, key_cache, value_cache))
    attended = attended.reshape(BATCH, HEADS * 2 * DH)
    attention_out = grouped_product(attended, out_weight, N_TP)
    mixed = (token_values + attention_out).astype(jnp.bfloat16)
    mixed_values = mixed.astype(jnp.float32)
    mixer_ratio = lax.rsqrt(lax.optimization_barrier(jnp.mean(mixed_values * mixed_values, axis=1, keepdims=True)) + NORM_EPSILON)
    mixer_scaled = (mixed_values * mixer_gain.astype(jnp.float32)).astype(jnp.bfloat16)
    gate_values = jnp.dot(mixer_scaled, gate_weight, preferred_element_type=jnp.float32) * mixer_ratio
    up_values = jnp.dot(mixer_scaled, up_weight, preferred_element_type=jnp.float32) * mixer_ratio
    hidden_state = (jax.nn.silu(gate_values) * up_values).astype(jnp.bfloat16)
    mixer_out = grouped_product(hidden_state, down_weight, N_TP)
    return (mixed_values + mixer_out).astype(jnp.bfloat16)
```

```python
import jax
import jax.numpy as jnp
import numpy as np
from jax import lax
from jax.experimental import pallas as pl
from jax.experimental.pallas import tpu as pltpu
from jax.sharding import PartitionSpec as P

MESH = pl.DeviceIdType.MESH
F32 = jnp.float32
BF16 = jnp.bfloat16

D = 2048
DH = 64
POSITIONS = 1024
HEADS = 4
ROWS = 8
KV = 16
FF = 2816
FT = FF // 128
HT = FT // 2
CACHE = KV * POSITIONS
NORM_EPSILON = 1e-06
HEAD_EPSILON = 1e-05
HEAD_SCALE = 0.8
FLOOR = -1e30
KEYS = POSITIONS * HEADS
QR = 33
CR = 72
GR = 24


def rotary_tables():
    half = DH // 2
    index = np.arange(half, dtype=np.float32) / np.float32(half)
    frequency = (np.float32(1.0) / np.power(np.float32(10000.0), index)).astype(np.float32)
    angle = (np.float32(CACHE) * frequency).astype(np.float32).astype(np.float64)
    cosine = np.tile(np.cos(angle).astype(np.float32), 4)
    sine = np.sin(angle).astype(np.float32)
    sine = np.tile(np.concatenate([-sine, sine]), 2)
    table = np.zeros((8, 128), np.float32)
    table[0], table[1] = cosine, sine
    return table


def layer_kernel(
    tok_h, ag_h, q1_h, q2_h, k1_h, k2_h, vw_h, hsw_h, hg_h, ow_h, mg_h, gw_h, uw_h, dw_h, kc_h, vc_h, tab_h,
    out_ref,
    tok_own, tok_far, ag_own, ag_far, mg_own, mg_far,
    q1_w, q2_w, k1_w, k2_w, vw_w, hsw, hg, ow_w, gw_w, uw_w, dw_w, kc, vc, tab,
    qx, ax, cx, gs, gx, hx, hs, qs, os_own, os_far, ds_own, ds_far,
    load_sem, pair_send, pair_recv, q_send, q_recv, a_send, a_recv, c_send, c_recv, g_send, g_recv, h_send, h_recv,
):
    dp, kv, tp = (lax.axis_index(a) for a in ("dp", "kv", "tp"))
    barrier = pltpu.get_barrier_semaphore()
    partner = (dp, kv, 1 - tp)
    peers = [lax.rem(kv + d, KV) for d in range(1, KV)]
    for p in peers:
        pl.semaphore_signal(barrier, 1, device_id=(dp, p, tp), device_id_type=MESH)
    pl.semaphore_signal(barrier, 1, device_id=partner, device_id_type=MESH)

    loads = []

    def load(src, dst):
        copy = pltpu.make_async_copy(src, dst, load_sem.at[len(loads)])
        copy.start()
        loads.append(copy)
        return copy

    first = [load(a, b) for a, b in ((tok_h, tok_own), (ag_h, ag_own), (mg_h, mg_own))]
    q_loads = [load(a, b) for a, b in ((q1_h, q1_w), (q2_h, q2_w), (tab_h, tab))]
    kv_loads = [load(a, b) for a, b in ((k1_h, k1_w), (k2_h, k2_w), (vw_h, vw_w))]
    k_loads = [load(kc_h.at[b], kc.at[b]) for b in range(ROWS)]
    v_loads = [load(vc_h.at[b], vc.at[b]) for b in range(ROWS)]
    late_loads = [
        load(a, b)
        for a, b in ((hsw_h, hsw), (hg_h, hg), (ow_h, ow_w), (gw_h, gw_w), (uw_h, uw_w), (dw_h, dw_w))
    ]
    for copy in first:
        copy.wait()
    pl.semaphore_wait(barrier, KV)

    sends = []

    def pair(k, src, dst):
        copy = pltpu.make_async_remote_copy(
            src, dst, pair_send.at[k], pair_recv.at[k], device_id=partner, device_id_type=MESH
        )
        copy.start()
        sends.append(copy)
        return copy

    def spread(source, landing, send_sem, recv_sem):
        for d, p in enumerate(peers):
            copy = pltpu.make_async_remote_copy(
                source(p), landing.at[kv], send_sem.at[d], recv_sem.at[kv],
                device_id=(dp, p, tp), device_id_type=MESH,
            )
            copy.start()
            sends.append(copy)

    def gathered(landing, recv_sem, send_sem):
        for d, p in enumerate(peers):
            pltpu.make_async_remote_copy(
                landing.at[p], landing.at[p], send_sem.at[d], recv_sem.at[p],
                device_id=(dp, p, tp), device_id_type=MESH,
            ).wait_recv()

    swaps = [pair(0, tok_own, tok_far), pair(1, ag_own, ag_far), pair(2, mg_own, mg_far)]
    lane = lax.broadcasted_iota(jnp.int32, (8, 128), 1)
    sub = lax.broadcasted_iota(jnp.int32, (8, 128), 0)
    diagonal = lane == sub
    for copy in q_loads:
        copy.wait()
    for copy in swaps:
        copy.wait_recv()

    def joined(own, far):
        own, far = own[...].astype(F32), far[...].astype(F32)
        return jnp.concatenate([jnp.where(tp == 0, own, far), jnp.where(tp == 0, far, own)], axis=-1)

    tokens = joined(tok_own, tok_far)
    scaled = (tokens * joined(ag_own, ag_far)).astype(BF16)
    mixer_gain = joined(mg_own, mg_far)
    square = jnp.sum(tokens * tokens, axis=1, keepdims=True)
    square_row = jnp.sum(jnp.where(diagonal, square, 0.0), axis=0, keepdims=True)
    for w, ref in enumerate((q1_w, q2_w)):
        part = jnp.dot(scaled, ref[...], preferred_element_type=F32)
        for t in range(2):
            qx[kv, 16 * w + 8 * t : 16 * w + 8 * t + 8, :] = part[:, 128 * t : 128 * t + 128]
    qx[kv, 32:33, :] = square_row
    spread(lambda p: qx.at[kv], qx, q_send, q_recv)

    for copy in kv_loads:
        copy.wait()
    for w, ref in enumerate((k1_w, k2_w)):
        part = jnp.dot(scaled, ref[...], preferred_element_type=F32)
        for t in range(2):
            ax[kv, 16 * w + 8 * t : 16 * w + 8 * t + 8, :] = part[:, 128 * t : 128 * t + 128]
    part = jnp.dot(scaled, vw_w[...], preferred_element_type=F32)
    for t in range(HEADS):
        ax[kv, 32 + 8 * t : 40 + 8 * t, :] = part[:, 128 * t : 128 * t + 128]
    spread(lambda p: ax.at[kv], ax, a_send, a_recv)

    gathered(qx, q_recv, q_send)

    def ratio_of(total):
        return lax.rsqrt(total / D + NORM_EPSILON)

    square_total = qx[0, 32:33, :]
    for s in range(1, KV):
        square_total = square_total + qx[s, 32:33, :]
    ratio_row = ratio_of(square_total)
    ratio = jnp.sum(jnp.where(diagonal, ratio_row, 0.0), axis=1, keepdims=True)
    cosine, sine = tab[0:1, :], tab[1:2, :]
    lead = lax.rem(lane, DH) < DH // 2

    def rotated(x):
        turned = jnp.where(lead, pltpu.roll(x, 128 - DH // 2, 1), pltpu.roll(x, DH // 2, 1))
        return (x * cosine + turned * sine).astype(BF16).astype(F32)

    def total_of(ref, at):
        total = ref[0, at : at + 8, :]
        for s in range(1, KV):
            total = total + ref[s, at : at + 8, :]
        return total

    query = [[rotated(total_of(qx, 16 * m + 8 * t) * ratio) for t in range(2)] for m in range(2)]
    low = lane < DH
    for h in range(HEADS):
        for m in range(2):
            x = query[m][h // 2]
            if h % 2 != m:
                x = pltpu.roll(x, DH, 1)
            qs[pl.ds(2 * h + m, 8, stride=8), :] = jnp.where(low if m == 0 else ~low, x, 0.0)

    key_head = lax.rem(lax.broadcasted_iota(jnp.int32, (16, 128), 1), HEADS)
    row_head = lax.rem(lax.broadcasted_iota(jnp.int32, (16, 128), 0), 8) // 2
    own_head = key_head == row_head
    scale = DH ** (-0.5)
    zero = jnp.zeros((8, 128), F32)
    peaks, sums = zero, zero
    for b in range(0, ROWS, 2):
        for copy in k_loads[b : b + 2]:
            copy.wait()
        left = jnp.concatenate(
            [
                jnp.concatenate([qs[8 * b : 8 * b + 8, :], zero], axis=1),
                jnp.concatenate([zero, qs[8 * b + 8 : 8 * b + 16, :]], axis=1),
            ],
            axis=0,
        ).astype(BF16)
        scores = []
        peak = jnp.full((16, 128), FLOOR, F32)
        step = 1024
        for c in range(0, KEYS, step):
            keys = jnp.concatenate([kc[b, c : c + step, :], kc[b + 1, c : c + step, :]], axis=1)
            s = lax.dot_general(left, keys, (((1,), (1,)), ((), ())), preferred_element_type=F32)
            for t in range(0, step, 128):
                one = jnp.where(own_head, s[:, t : t + 128], FLOOR)
                peak = jnp.maximum(peak, one)
                scores.append(one)
        peak = jnp.max(peak, axis=1, keepdims=True)
        total = jnp.zeros((16, 128), F32)
        weights = []
        for one in scores:
            e = jnp.exp((one - peak) * scale)
            total = total + e
            weights.append(e.astype(BF16))
        total = jnp.sum(total, axis=1, keepdims=True)
        for copy in v_loads[b : b + 2]:
            copy.wait()
        acc = jnp.zeros((16, 256), F32)
        for c in range(0, KEYS, step):
            values = jnp.concatenate([vc[b, c : c + step, :], vc[b + 1, c : c + step, :]], axis=1)
            w = jnp.concatenate(weights[c // 128 : (c + step) // 128], axis=1)
            acc = acc + jnp.dot(w, values, preferred_element_type=F32)
        for k in range(2):
            at = 8 * k
            cx[kv, pl.ds(b + k, 8, stride=8), :] = acc[at : at + 8, 128 * k : 128 * k + 128]
            for value, base in ((peak * scale, 0), (total, 8)):
                column = value[at : at + 8]
                row = jnp.sum(jnp.where(lane - base == sub, column, 0.0), axis=0, keepdims=True)
                if base == 0:
                    peaks = jnp.where(sub == b + k, row, peaks)
                else:
                    sums = jnp.where(sub == b + k, row, sums)
    cx[kv, 64:72, :] = jnp.where(lane < 8, peaks, sums)
    spread(lambda p: cx.at[kv], cx, c_send, c_recv)

    gathered(ax, a_recv, a_send)
    own_scores, new_values = [], []
    for m in range(2):
        for t in range(2):
            product = query[m][t] * rotated(total_of(ax, 16 * m + 8 * t) * ratio)
            for k in range(2):
                half = jnp.sum(jnp.where(low if k == 0 else ~low, product, 0.0), axis=1, keepdims=True)
                own_scores.append((2 * t + k, m, half * scale))
    own_scores = {(h, m): s for h, m, s in own_scores}
    for h in range(HEADS):
        new_values.append((total_of(ax, 32 + 8 * h) * ratio).astype(BF16).astype(F32))
    own = zero
    for h in range(HEADS):
        for m in range(2):
            own = jnp.where(lane == 2 * h + m, own_scores[h, m], own)
    for copy in late_loads[:3]:
        copy.wait()

    gathered(cx, c_recv, c_send)
    stats = [cx[s, 64:72, :] for s in range(KV)]
    peak = own
    for s in stats:
        peak = jnp.maximum(peak, s)
    own_weight = jnp.exp(own - peak)
    factors = [jnp.exp(s - peak) for s in stats]
    weight_sum = own_weight
    for f, s in zip(factors, stats):
        weight_sum = weight_sum + f * pltpu.roll(s, 120, 1)
    inverse = 1.0 / weight_sum
    attended = []
    for h in range(HEADS):
        averaged = []
        for m in range(2):
            c = 2 * h + m
            acc = own_weight[:, c : c + 1] * new_values[h]
            for s in range(KV):
                acc = acc + factors[s][:, c : c + 1] * cx[s, 8 * c : 8 * c + 8, :]
            averaged.append(acc * inverse[:, c : c + 1])
        difference = averaged[0] - hsw[0:1, h : h + 1] * averaged[1]
        norm = lax.rsqrt(jnp.mean(difference * difference, axis=1, keepdims=True) + HEAD_EPSILON)
        attended.append((difference * norm * hg[...] * HEAD_SCALE).astype(BF16))
    attended = jnp.concatenate(attended, axis=1)
    os_own[...] = jnp.dot(attended, ow_w[...], preferred_element_type=F32).astype(BF16)
    swap = pair(3, os_own, os_far)
    for copy in late_loads[3:]:
        copy.wait()
    swap.wait_recv()
    mixed = (tokens + (os_own[...].astype(F32) + os_far[...].astype(F32))).astype(BF16).astype(F32)
    mixer_scaled = (mixed * mixer_gain).astype(BF16)
    square = jnp.broadcast_to(jnp.sum(mixed * mixed, axis=1, keepdims=True), (8, 128))
    for w, ref in enumerate((gw_w, uw_w)):
        part = jnp.dot(mixer_scaled, ref[...], preferred_element_type=F32)
        for t in range(FT):
            row = (t // HT) * GR + w * HT + t % HT
            gs[pl.ds(row, 8, stride=2 * GR), :] = part[:, 128 * t : 128 * t + 128]
    for half in range(2):
        gs[pl.ds(half * GR + 2 * HT, 8, stride=2 * GR), :] = square
    gx[kv] = gs[pl.ds(pl.multiple_of(kv * GR, 8), GR), :]
    spread(lambda p: gs.at[pl.ds(pl.multiple_of(p * GR, 8), GR), :], gx, g_send, g_recv)
    gathered(gx, g_recv, g_send)
    total = gx[0]
    for s in range(1, KV):
        total = total + gx[s]
    mixer_ratio = ratio_of(total[2 * HT : 2 * HT + 1])
    gate = total[:HT] * mixer_ratio
    up = total[HT : 2 * HT] * mixer_ratio
    hidden = gate / (1.0 + jnp.exp(-gate)) * up
    hx[kv, 0:HT, :] = hidden.astype(BF16)
    spread(lambda p: hx.at[kv], hx, h_send, h_recv)
    gathered(hx, h_recv, h_send)
    for s in range(KV):
        hs[16 * s : 16 * s + 16, :] = hx[s].astype(F32)
    hidden = jnp.concatenate(
        [hs[pl.ds(16 * (t // HT) + t % HT, 8, stride=32), :].astype(BF16) for t in range(FT)], axis=1
    )
    ds_own[...] = jnp.dot(hidden, dw_w[...], preferred_element_type=F32).astype(BF16)
    swap = pair(4, ds_own, ds_far)
    swap.wait_recv()
    result = mixed + (ds_own[...].astype(F32) + ds_far[...].astype(F32))
    result = jnp.where(tp == 0, result, pltpu.roll(result, DH, 1))
    out_ref[...] = result[:, :64].astype(BF16)
    for copy in sends:
        copy.wait_send()


def shards(
    tokens, attention_gain, query_one, query_two, key_one, key_two, value_weight, head_second_weight, head_gain,
    out_weight, mixer_gain, gate_weight, up_weight, down_weight, key_cache, value_cache,
):
    any_space = pl.BlockSpec(memory_space=pl.ANY)
    vmem = pltpu.VMEM
    dma = pltpu.SemaphoreType.DMA
    return pl.pallas_call(
        layer_kernel,
        out_shape=jax.ShapeDtypeStruct((ROWS, 64), BF16),
        in_specs=[any_space] * 17,
        out_specs=pl.BlockSpec(memory_space=pltpu.VMEM),
        scratch_shapes=[
            vmem((ROWS, 64), BF16), vmem((ROWS, 64), BF16),
            vmem((1, 64), BF16), vmem((1, 64), BF16), vmem((1, 64), BF16), vmem((1, 64), BF16),
            vmem((128, 256), BF16), vmem((128, 256), BF16), vmem((128, 256), BF16), vmem((128, 256), BF16),
            vmem((128, 512), BF16), vmem((1, HEADS), F32), vmem((1, 128), F32), vmem((512, 128), BF16),
            vmem((128, FF), BF16), vmem((128, FF), BF16), vmem((FF, 128), BF16),
            vmem((ROWS, KEYS, 128), BF16), vmem((ROWS, KEYS, 128), BF16), vmem((8, 128), F32),
            vmem((KV, QR, 128), F32), vmem((KV, 64, 128), F32), vmem((KV, CR, 128), F32),
            vmem((KV * GR, 128), F32), vmem((KV, GR, 128), F32),
            vmem((KV, 16, 128), BF16), vmem((KV * 16, 128), F32), vmem((64, 128), F32),
            vmem((8, 128), BF16), vmem((8, 128), BF16), vmem((8, 128), BF16), vmem((8, 128), BF16),
            dma((31,)), dma((5,)), dma((5,)),
            dma((KV,)), dma((KV,)), dma((KV,)), dma((KV,)), dma((KV,)), dma((KV,)),
            dma((KV,)), dma((KV,)), dma((KV,)), dma((KV,)),
        ],
        compiler_params=pltpu.CompilerParams(
            collective_id=0, has_side_effects=True, vmem_limit_bytes=60 * 1024 * 1024
        ),
        name="layer",
    )(
        tokens, attention_gain.reshape(1, -1), query_one, query_two, key_one, key_two, value_weight,
        head_second_weight.reshape(1, -1), head_gain.reshape(1, -1), out_weight, mixer_gain.reshape(1, -1),
        gate_weight, up_weight, down_weight,
        key_cache.reshape(ROWS, KEYS, 128), value_cache.reshape(ROWS, KEYS, 128), jnp.asarray(rotary_tables()),
    )


def solution(mesh):
    both = ("kv", "tp")
    return jax.shard_map(
        shards,
        mesh=mesh,
        in_specs=(
            P("dp", both), P(both), P("kv", "tp"), P("kv", "tp"), P("kv", "tp"), P("kv", "tp"), P("kv", "tp"),
            P("tp"), P(), P("tp", "kv"), P(both), P("kv", "tp"), P("kv", "tp"), P("tp", "kv"),
            P("dp", "kv", "tp", None), P("dp", "kv", "tp", None),
        ),
        out_specs=P("dp", both),
        check_vma=False,
    )
```

```python
import jax
import jax.numpy as jnp
import numpy as np
from jax import lax
from jax.experimental import pallas as pl
from jax.experimental.pallas import tpu as pltpu
from jax.sharding import PartitionSpec as P

MESH = pl.DeviceIdType.MESH
F32 = jnp.float32
BF16 = jnp.bfloat16

D = 2048
DH = 64
POSITIONS = 1024
HEADS = 4
ROWS = 8
KV = 16
FF = 2816
FT = FF // 128
HT = FT // 2
CACHE = KV * POSITIONS
NORM_EPSILON = 1e-06
HEAD_EPSILON = 1e-05
HEAD_SCALE = 0.8
FLOOR = -1e30
KEYS = POSITIONS * HEADS
QR = 33
GR = 24


def rotary_tables():
    half = DH // 2
    index = np.arange(half, dtype=np.float32) / np.float32(half)
    frequency = (np.float32(1.0) / np.power(np.float32(10000.0), index)).astype(np.float32)
    angle = (np.float32(CACHE) * frequency).astype(np.float32).astype(np.float64)
    cosine = np.tile(np.cos(angle).astype(np.float32), 4)
    sine = np.sin(angle).astype(np.float32)
    sine = np.tile(np.concatenate([-sine, sine]), 2)
    table = np.zeros((8, 128), np.float32)
    table[0], table[1] = cosine, sine
    return table


def layer_kernel(
    tok_h, ag_h, q1_h, q2_h, k1_h, k2_h, vw_h, hsw_h, hg_h, ow_h, mg_h, gw_h, uw_h, dw_h, kc_h, vc_h, tab_h,
    out_ref,
    tok_own, tok_far, ag_own, ag_far, mg_own, mg_far,
    q1_w, q2_w, k1_w, k2_w, vw_w, hsw, hg, ow_w, gw_w, uw_w, dw_w, kc, vc, tab,
    qx, rs, rx, nx, cx, sx, gs, gx, hx, hs, qs, nv, sc, df, os_own, os_far, ds_own, ds_far,
    load_sem, pair_send, pair_recv, all_send, all_recv,
):
    dp, kv, tp = (lax.axis_index(a) for a in ("dp", "kv", "tp"))
    barrier = pltpu.get_barrier_semaphore()
    partner = (dp, kv, 1 - tp)
    peers = [lax.rem(kv + d, KV) for d in range(1, KV)]
    for p in peers:
        pl.semaphore_signal(barrier, 1, device_id=(dp, p, tp), device_id_type=MESH)
    pl.semaphore_signal(barrier, 1, device_id=partner, device_id_type=MESH)

    loads = []

    def load(src, dst):
        copy = pltpu.make_async_copy(src, dst, load_sem.at[len(loads)])
        copy.start()
        loads.append(copy)
        return copy

    first = [load(a, b) for a, b in ((tok_h, tok_own), (ag_h, ag_own), (mg_h, mg_own))]
    q_loads = [load(a, b) for a, b in ((q1_h, q1_w), (q2_h, q2_w), (tab_h, tab))]
    kv_loads = [load(a, b) for a, b in ((k1_h, k1_w), (k2_h, k2_w), (vw_h, vw_w))]
    cache_loads = [load(kc_h, kc), load(vc_h, vc)]
    late_loads = [
        load(a, b)
        for a, b in ((hsw_h, hsw), (hg_h, hg), (ow_h, ow_w), (gw_h, gw_w), (uw_h, uw_w), (dw_h, dw_w))
    ]
    for copy in first:
        copy.wait()
    pl.semaphore_wait(barrier, KV)

    sends, spreads = [], []

    def pair(k, src, dst):
        copy = pltpu.make_async_remote_copy(
            src, dst, pair_send.at[k], pair_recv.at[k], device_id=partner, device_id_type=MESH
        )
        copy.start()
        sends.append(copy)
        return copy

    def spread(stage, source, target):
        for p in peers:
            pltpu.make_async_remote_copy(
                source(p), target, all_send.at[stage], all_recv.at[stage],
                device_id=(dp, p, tp), device_id_type=MESH,
            ).start()

    def everything(stage, landing):
        most = landing.at[0 : KV - 1]
        copy = pltpu.make_async_remote_copy(
            most, most, all_send.at[stage], all_recv.at[stage], device_id=partner, device_id_type=MESH
        )
        spreads.append(copy)
        copy.wait_recv()

    swaps = [pair(0, tok_own, tok_far), pair(1, ag_own, ag_far), pair(2, mg_own, mg_far)]
    lane = lax.broadcasted_iota(jnp.int32, (8, 128), 1)
    sub = lax.broadcasted_iota(jnp.int32, (8, 128), 0)
    diagonal = lane == sub
    for copy in q_loads:
        copy.wait()
    for copy in swaps:
        copy.wait_recv()

    def joined(own, far):
        own, far = own[...].astype(F32), far[...].astype(F32)
        return jnp.concatenate([jnp.where(tp == 0, own, far), jnp.where(tp == 0, far, own)], axis=-1)

    tokens = joined(tok_own, tok_far)
    scaled = (tokens * joined(ag_own, ag_far)).astype(BF16)
    mixer_gain = joined(mg_own, mg_far)
    square = jnp.sum(tokens * tokens, axis=1, keepdims=True)
    square_row = jnp.sum(jnp.where(diagonal, square, 0.0), axis=0, keepdims=True)
    for w, ref in enumerate((q1_w, q2_w)):
        part = jnp.dot(scaled, ref[...], preferred_element_type=F32)
        for t in range(2):
            qx[kv, 16 * w + 8 * t : 16 * w + 8 * t + 8, :] = part[:, 128 * t : 128 * t + 128]
    qx[kv, 32:33, :] = square_row
    spread(0, lambda p: qx.at[kv], qx.at[kv])

    for copy in kv_loads:
        copy.wait()
    for w, ref in enumerate((k1_w, k2_w)):
        part = jnp.dot(scaled, ref[...], preferred_element_type=F32)
        for t in range(2):
            rs[pl.ds(8 * t + w, 8, stride=16), :] = part[:, 128 * t : 128 * t + 128]
    part = jnp.dot(scaled, vw_w[...], preferred_element_type=F32)
    for t in range(HEADS):
        rs[pl.ds(8 * (t // 2) + 2 + t % 2, 8, stride=16), :] = part[:, 128 * t : 128 * t + 128]
    rx[kv] = rs[pl.ds(pl.multiple_of(8 * kv, 8), 8), :]
    spread(1, lambda p: rs.at[pl.ds(pl.multiple_of(8 * p, 8), 8), :], rx.at[kv])

    for copy in cache_loads:
        copy.wait()
    everything(0, qx)

    def ratio_of(total):
        return lax.rsqrt(total / D + NORM_EPSILON)

    square_total = qx[0, 32:33, :]
    for s in range(1, KV):
        square_total = square_total + qx[s, 32:33, :]
    ratio_row = ratio_of(square_total)
    ratio = jnp.sum(jnp.where(diagonal, ratio_row, 0.0), axis=1, keepdims=True)
    cosine, sine = tab[0:1, :], tab[1:2, :]
    lead = lax.rem(lane, DH) < DH // 2

    def rotated(x):
        turned = jnp.where(lead, pltpu.roll(x, 128 - DH // 2, 1), pltpu.roll(x, DH // 2, 1))
        return (x * cosine + turned * sine).astype(BF16).astype(F32)

    def total_of(ref, at):
        total = ref[0, at : at + 8, :]
        for s in range(1, KV):
            total = total + ref[s, at : at + 8, :]
        return total

    query = [[rotated(total_of(qx, 16 * m + 8 * t) * ratio) for t in range(2)] for m in range(2)]
    low = lane < DH
    for h in range(HEADS):
        for m in range(2):
            x = query[m][h // 2]
            if h % 2 != m:
                x = pltpu.roll(x, DH, 1)
            qs[pl.ds(2 * h + m, 8, stride=8), :] = jnp.where(low if m == 0 else ~low, x, 0.0)

    key_head = lax.rem(lax.broadcasted_iota(jnp.int32, (16, 128), 1), HEADS)
    row_head = lax.rem(lax.broadcasted_iota(jnp.int32, (16, 128), 0), 8) // 2
    own_head = key_head == row_head
    scale = DH ** (-0.5)
    zero = jnp.zeros((8, 128), F32)
    step = 1024

    def score(pair_index):
        b = 2 * pair_index
        left = jnp.concatenate(
            [
                jnp.concatenate([qs[8 * b : 8 * b + 8, :], zero], axis=1),
                jnp.concatenate([zero, qs[8 * b + 8 : 8 * b + 16, :]], axis=1),
            ],
            axis=0,
        ).astype(BF16)
        peak = jnp.full((16, 128), FLOOR, F32)
        for c in range(0, KEYS, step):
            keys = jnp.concatenate([kc[b, c : c + step, :], kc[b + 1, c : c + step, :]], axis=1)
            s = lax.dot_general(left, keys, (((1,), (1,)), ((), ())), preferred_element_type=F32)
            for t in range(0, step, 128):
                one = jnp.where(own_head, s[:, t : t + 128], FLOOR)
                peak = jnp.maximum(peak, one)
                sc[pair_index % 2, :, c + t : c + t + 128] = one
        return peak

    stat = zero
    running = score(0)
    for pair_index in range(ROWS // 2):
        b = 2 * pair_index
        peak = jnp.max(running, axis=1, keepdims=True)
        if pair_index + 1 < ROWS // 2:
            running = score(pair_index + 1)
        total = jnp.zeros((16, 128), F32)
        weights = []
        for t in range(0, KEYS, 128):
            e = jnp.exp((sc[pair_index % 2, :, t : t + 128] - peak) * scale)
            total = total + e
            weights.append(e.astype(BF16))
        total = jnp.sum(total, axis=1, keepdims=True)
        for k in range(2):
            stat = jnp.where(lane == b + k, peak[8 * k : 8 * k + 8] * scale, stat)
            stat = jnp.where(lane == 8 + b + k, total[8 * k : 8 * k + 8], stat)
        if pair_index + 1 == ROWS // 2:
            sx[kv] = stat
            spread(2, lambda p: sx.at[kv], sx.at[kv])
        acc = jnp.zeros((16, 256), F32)
        for c in range(0, KEYS, step):
            values = jnp.concatenate([vc[b, c : c + step, :], vc[b + 1, c : c + step, :]], axis=1)
            w = jnp.concatenate(weights[c // 128 : (c + step) // 128], axis=1)
            acc = acc + jnp.dot(w, values, preferred_element_type=F32)
        place = pl.ds(8 * b, 16)
        cx[kv, place, :] = jnp.concatenate([acc[0:8, 0:128], acc[8:16, 128:256]], axis=0).astype(BF16)
        spread(3, lambda p: cx.at[kv, place], cx.at[kv, place])
        if pair_index == 1:
            everything(1, rx)
            nx[pl.ds(pl.multiple_of(8 * kv, 8), 8), :] = total_of(rx, 0)
            mine = nx.at[pl.ds(pl.multiple_of(8 * kv, 8), 8), :]
            spread(4, lambda p: mine, mine)

    most = nx.at[0 : 8 * (KV - 1)]
    copy = pltpu.make_async_remote_copy(
        most, most, all_send.at[4], all_recv.at[4], device_id=partner, device_id_type=MESH
    )
    spreads.append(copy)
    copy.wait_recv()
    own = zero
    for m in range(2):
        for t in range(2):
            product = query[m][t] * rotated(nx[pl.ds(8 * t + m, 8, stride=16), :] * ratio)
            for k in range(2):
                half = jnp.sum(jnp.where(low if k == 0 else ~low, product, 0.0), axis=1, keepdims=True)
                row = jnp.sum(jnp.where(diagonal, half, 0.0), axis=0, keepdims=True)
                own = jnp.where(sub == 2 * (2 * t + k) + m, row * scale, own)
    for h in range(HEADS):
        value = (nx[pl.ds(8 * (h // 2) + 2 + h % 2, 8, stride=16), :] * ratio).astype(BF16).astype(F32)
        for m in range(2):
            nv[pl.ds(2 * h + m, 8, stride=8), :] = value
    for copy in late_loads[:3]:
        copy.wait()
    second = jnp.zeros((8, 1), F32)
    for h in range(HEADS):
        second = jnp.where(sub[:, :1] == 2 * h, hsw[0:1, h : h + 1], second)

    everything(2, sx)
    stats = [sx[s] for s in range(KV)]
    peak = own
    for s in stats:
        peak = jnp.maximum(peak, s)
    own_weight = jnp.exp(own - peak)
    factors = [jnp.exp(s - peak) for s in stats]
    weight_sum = own_weight
    for f, s in zip(factors, stats):
        weight_sum = weight_sum + f * pltpu.roll(s, 120, 1)
    inverse = 1.0 / weight_sum
    everything(3, cx)
    for b in range(0, ROWS, 2):
        acc = [own_weight[:, b + k : b + k + 1] * nv[8 * (b + k) : 8 * (b + k) + 8, :] for k in range(2)]
        for s in range(KV):
            part = cx[s, 8 * b : 8 * b + 16, :].astype(F32)
            for k in range(2):
                acc[k] = acc[k] + factors[s][:, b + k : b + k + 1] * part[8 * k : 8 * k + 8]
        for k in range(2):
            averaged = acc[k] * inverse[:, b + k : b + k + 1]
            difference = averaged - second * pltpu.roll(averaged, 7, 0)
            norm = lax.rsqrt(jnp.mean(difference * difference, axis=1, keepdims=True) + HEAD_EPSILON)
            df[8 * (b + k) : 8 * (b + k) + 8, :] = difference * norm * hg[...] * HEAD_SCALE
    attended = jnp.concatenate([df[pl.ds(2 * h, 8, stride=8), :].astype(BF16) for h in range(HEADS)], axis=1)
    os_own[...] = jnp.dot(attended, ow_w[...], preferred_element_type=F32).astype(BF16)
    swap = pair(3, os_own, os_far)
    for copy in late_loads[3:]:
        copy.wait()
    swap.wait_recv()
    mixed = (tokens + (os_own[...].astype(F32) + os_far[...].astype(F32))).astype(BF16).astype(F32)
    mixer_scaled = (mixed * mixer_gain).astype(BF16)
    square = jnp.broadcast_to(jnp.sum(mixed * mixed, axis=1, keepdims=True), (8, 128))
    for w, ref in enumerate((gw_w, uw_w)):
        part = jnp.dot(mixer_scaled, ref[...], preferred_element_type=F32)
        for t in range(FT):
            row = (t // HT) * GR + w * HT + t % HT
            gs[pl.ds(row, 8, stride=2 * GR), :] = part[:, 128 * t : 128 * t + 128]
    for half in range(2):
        gs[pl.ds(half * GR + 2 * HT, 8, stride=2 * GR), :] = square
    gx[kv] = gs[pl.ds(pl.multiple_of(kv * GR, 8), GR), :]
    spread(5, lambda p: gs.at[pl.ds(pl.multiple_of(p * GR, 8), GR), :], gx.at[kv])
    everything(5, gx)
    total = gx[0]
    for s in range(1, KV):
        total = total + gx[s]
    mixer_ratio = ratio_of(total[2 * HT : 2 * HT + 1])
    gate = total[:HT] * mixer_ratio
    up = total[HT : 2 * HT] * mixer_ratio
    hidden = gate / (1.0 + jnp.exp(-gate)) * up
    hx[kv, 0:HT, :] = hidden.astype(BF16)
    spread(6, lambda p: hx.at[kv], hx.at[kv])
    everything(6, hx)
    for s in range(KV):
        hs[16 * s : 16 * s + 16, :] = hx[s].astype(F32)
    hidden = jnp.concatenate(
        [hs[pl.ds(16 * (t // HT) + t % HT, 8, stride=32), :].astype(BF16) for t in range(FT)], axis=1
    )
    ds_own[...] = jnp.dot(hidden, dw_w[...], preferred_element_type=F32).astype(BF16)
    swap = pair(4, ds_own, ds_far)
    swap.wait_recv()
    result = mixed + (ds_own[...].astype(F32) + ds_far[...].astype(F32))
    result = jnp.where(tp == 0, result, pltpu.roll(result, DH, 1))
    out_ref[...] = result[:, :64].astype(BF16)
    for copy in sends + spreads:
        copy.wait_send()


def shards(
    tokens, attention_gain, query_one, query_two, key_one, key_two, value_weight, head_second_weight, head_gain,
    out_weight, mixer_gain, gate_weight, up_weight, down_weight, key_cache, value_cache,
):
    any_space = pl.BlockSpec(memory_space=pl.ANY)
    vmem = pltpu.VMEM
    dma = pltpu.SemaphoreType.DMA
    return pl.pallas_call(
        layer_kernel,
        out_shape=jax.ShapeDtypeStruct((ROWS, 64), BF16),
        in_specs=[any_space] * 17,
        out_specs=pl.BlockSpec(memory_space=pltpu.VMEM),
        scratch_shapes=[
            vmem((ROWS, 64), BF16), vmem((ROWS, 64), BF16),
            vmem((1, 64), BF16), vmem((1, 64), BF16), vmem((1, 64), BF16), vmem((1, 64), BF16),
            vmem((128, 256), BF16), vmem((128, 256), BF16), vmem((128, 256), BF16), vmem((128, 256), BF16),
            vmem((128, 512), BF16), vmem((1, HEADS), F32), vmem((1, 128), F32), vmem((512, 128), BF16),
            vmem((128, FF), BF16), vmem((128, FF), BF16), vmem((FF, 128), BF16),
            vmem((ROWS, KEYS, 128), BF16), vmem((ROWS, KEYS, 128), BF16), vmem((8, 128), F32),
            vmem((KV, QR, 128), F32), vmem((KV * 8, 128), F32), vmem((KV, 8, 128), F32), vmem((KV * 8, 128), F32),
            vmem((KV, 64, 128), BF16), vmem((KV, 8, 128), F32),
            vmem((KV * GR, 128), F32), vmem((KV, GR, 128), F32),
            vmem((KV, 16, 128), BF16), vmem((KV * 16, 128), F32), vmem((64, 128), F32), vmem((64, 128), F32),
            vmem((2, 16, KEYS), F32), vmem((64, 128), F32),
            vmem((8, 128), BF16), vmem((8, 128), BF16), vmem((8, 128), BF16), vmem((8, 128), BF16),
            dma((17,)), dma((5,)), dma((5,)), dma((7,)), dma((7,)),
        ],
        compiler_params=pltpu.CompilerParams(
            collective_id=0, has_side_effects=True, vmem_limit_bytes=60 * 1024 * 1024
        ),
        name="layer",
    )(
        tokens, attention_gain.reshape(1, -1), query_one, query_two, key_one, key_two, value_weight,
        head_second_weight.reshape(1, -1), head_gain.reshape(1, -1), out_weight, mixer_gain.reshape(1, -1),
        gate_weight, up_weight, down_weight,
        key_cache.reshape(ROWS, KEYS, 128), value_cache.reshape(ROWS, KEYS, 128), jnp.asarray(rotary_tables()),
    )


def solution(mesh):
    both = ("kv", "tp")
    return jax.shard_map(
        shards,
        mesh=mesh,
        in_specs=(
            P("dp", both), P(both), P("kv", "tp"), P("kv", "tp"), P("kv", "tp"), P("kv", "tp"), P("kv", "tp"),
            P("tp"), P(), P("tp", "kv"), P(both), P("kv", "tp"), P("kv", "tp"), P("tp", "kv"),
            P("dp", "kv", "tp", None), P("dp", "kv", "tp", None),
        ),
        out_specs=P("dp", both),
        check_vma=False,
    )
```

```python
import jax
import jax.numpy as jnp
import numpy as np
from jax import lax
from jax.experimental import pallas as pl
from jax.experimental.pallas import tpu as pltpu
from jax.sharding import PartitionSpec as P

MESH = pl.DeviceIdType.MESH
F32 = jnp.float32
BF16 = jnp.bfloat16

D = 2048
DH = 64
POSITIONS = 1024
HEADS = 4
ROWS = 8
KV = 16
FF = 2816
FT = FF // 128
HT = FT // 2
CACHE = KV * POSITIONS
NORM_EPSILON = 1e-06
HEAD_EPSILON = 1e-05
HEAD_SCALE = 0.8
FLOOR = -1e30
LOG2E = 1.4426950408889634
KEYS = POSITIONS * HEADS
QR = 33
GR = 24


OFFSETS = sorted(
    ((i, j) for i in range(4) for j in range(4) if (i, j) != (0, 0)),
    key=lambda o: -min(o[0], 4 - o[0]) - min(o[1], 4 - o[1]),
)


def rotary_tables():
    half = DH // 2
    index = np.arange(half, dtype=np.float32) / np.float32(half)
    frequency = (np.float32(1.0) / np.power(np.float32(10000.0), index)).astype(np.float32)
    angle = (np.float32(CACHE) * frequency).astype(np.float32).astype(np.float64)
    cosine = np.tile(np.cos(angle).astype(np.float32), 4)
    sine = np.sin(angle).astype(np.float32)
    sine = np.tile(np.concatenate([-sine, sine]), 2)
    table = np.zeros((8, 128), np.float32)
    table[0], table[1] = cosine, sine
    return table


def layer_kernel(
    tok_h, ag_h, q1_h, q2_h, k1_h, k2_h, vw_h, hsw_h, hg_h, ow_h, mg_h, gw_h, uw_h, dw_h, kc_h, vc_h, tab_h,
    out_ref,
    tok_own, tok_far, ag_own, ag_far, mg_own, mg_far,
    q1_w, q2_w, k1_w, k2_w, vw_w, hsw, hg, ow_w, gw_w, uw_w, dw_w, kc, vc, tab,
    unit, kt, qx, rs, rx, cx, sx, gs, gb, gx, hx, hs, qs, sc, df, os_own, os_far, ds_own, ds_far, out_v,
    load_sem, pair_send, pair_recv, all_send, all_recv,
):
    dp, kv, tp = (lax.axis_index(a) for a in ("dp", "kv", "tp"))
    barrier = pltpu.get_barrier_semaphore()
    partner = (dp, kv, 1 - tp)
    across, along = kv // 4, lax.rem(kv, 4)
    peers = [lax.rem(across + i, 4) * 4 + lax.rem(along + j, 4) for i, j in OFFSETS]
    for p in peers:
        pl.semaphore_signal(barrier, 1, device_id=(dp, p, tp), device_id_type=MESH)
    pl.semaphore_signal(barrier, 1, device_id=partner, device_id_type=MESH)

    loads = []

    def load(src, dst):
        copy = pltpu.make_async_copy(src, dst, load_sem.at[len(loads)])
        copy.start()
        loads.append(copy)
        return copy

    first = [load(a, b) for a, b in ((tok_h, tok_own), (ag_h, ag_own), (mg_h, mg_own))]
    q_loads = [load(a, b) for a, b in ((q1_h, q1_w), (q2_h, q2_w), (tab_h, tab))]
    kv_loads = [load(a, b) for a, b in ((k1_h, k1_w), (k2_h, k2_w), (vw_h, vw_w))]
    cache_loads = [load(kc_h, kc), load(vc_h, vc)]
    late_loads = [
        load(a, b)
        for a, b in ((hsw_h, hsw), (hg_h, hg), (ow_h, ow_w), (gw_h, gw_w), (uw_h, uw_w), (dw_h, dw_w))
    ]
    for copy in first:
        copy.wait()
    pl.semaphore_wait(barrier, KV)

    sends, spreads = [], []

    def pair(k, src, dst):
        copy = pltpu.make_async_remote_copy(
            src, dst, pair_send.at[k], pair_recv.at[k], device_id=partner, device_id_type=MESH
        )
        copy.start()
        sends.append(copy)
        return copy

    def spread(stage, source, target):
        for p in peers:
            pltpu.make_async_remote_copy(
                source(p), target, all_send.at[stage], all_recv.at[stage],
                device_id=(dp, p, tp), device_id_type=MESH,
            ).start()

    def everything(stage, most):
        copy = pltpu.make_async_remote_copy(
            most, most, all_send.at[stage], all_recv.at[stage], device_id=partner, device_id_type=MESH
        )
        spreads.append(copy)
        copy.wait_recv()

    swaps = [pair(0, tok_own, tok_far), pair(1, ag_own, ag_far), pair(2, mg_own, mg_far)]
    lane = lax.broadcasted_iota(jnp.int32, (8, 128), 1)
    sub = lax.broadcasted_iota(jnp.int32, (8, 128), 0)
    diagonal = lane == sub
    for copy in q_loads:
        copy.wait()
    for copy in swaps:
        copy.wait_recv()

    def joined(own, far):
        own, far = own[...].astype(F32), far[...].astype(F32)
        return jnp.concatenate([jnp.where(tp == 0, own, far), jnp.where(tp == 0, far, own)], axis=-1)

    tokens = joined(tok_own, tok_far)
    scaled = (tokens * joined(ag_own, ag_far)).astype(BF16)
    mixer_gain = joined(mg_own, mg_far)
    square = jnp.sum(tokens * tokens, axis=1, keepdims=True)
    square_row = jnp.sum(jnp.where(diagonal, square, 0.0), axis=0, keepdims=True)
    for w, ref in enumerate((q1_w, q2_w)):
        part = jnp.dot(scaled, ref[...], preferred_element_type=F32)
        for t in range(2):
            qx[kv, 16 * w + 8 * t : 16 * w + 8 * t + 8, :] = part[:, 128 * t : 128 * t + 128]
    qx[kv, 32:33, :] = square_row
    spread(0, lambda p: qx.at[kv], qx.at[kv])

    for copy in kv_loads:
        copy.wait()
    for w, ref in enumerate((k1_w, k2_w)):
        part = jnp.dot(scaled, ref[...], preferred_element_type=F32)
        for t in range(2):
            rs[pl.ds(8 * t + w, 8, stride=16), :] = part[:, 128 * t : 128 * t + 128]
    part = jnp.dot(scaled, vw_w[...], preferred_element_type=F32)
    for t in range(HEADS):
        rs[pl.ds(8 * (t // 2) + 2 + t % 2, 8, stride=16), :] = part[:, 128 * t : 128 * t + 128]
    rx[kv] = rs[pl.ds(pl.multiple_of(8 * kv, 8), 8), :]
    spread(1, lambda p: rs.at[pl.ds(pl.multiple_of(8 * p, 8), 4), :], rx.at[kv, 0:4])

    wide = (256, 256)
    unit[...] = (lax.broadcasted_iota(jnp.int32, wide, 0) == lax.broadcasted_iota(jnp.int32, wide, 1)).astype(BF16)
    cache_loads[0].wait()

    def turn(c, carry):
        at = pl.multiple_of(c * 512, 512)
        for b in range(0, ROWS, 2):
            keys = jnp.concatenate([kc[b, pl.ds(at, 512), :], kc[b + 1, pl.ds(at, 512), :]], axis=1)
            turned = lax.dot_general(unit[...], keys, (((1,), (1,)), ((), ())), preferred_element_type=F32)
            kt[b // 2, :, pl.ds(at, 512)] = turned.astype(BF16)
        return carry

    lax.fori_loop(0, KEYS // 512, turn, 0)
    cache_loads[1].wait()
    everything(0, qx.at[0 : KV - 1])

    def ratio_of(total):
        return lax.rsqrt(total / D + NORM_EPSILON)

    square_total = qx[0, 32:33, :]
    for s in range(1, KV):
        square_total = square_total + qx[s, 32:33, :]
    ratio_row = ratio_of(square_total)
    ratio = jnp.sum(jnp.where(diagonal, ratio_row, 0.0), axis=1, keepdims=True)
    cosine, sine = tab[0:1, :], tab[1:2, :]
    lead = lax.rem(lane, DH) < DH // 2

    def rotated(x):
        turned = jnp.where(lead, pltpu.roll(x, 128 - DH // 2, 1), pltpu.roll(x, DH // 2, 1))
        return (x * cosine + turned * sine).astype(BF16).astype(F32)

    def total_of(ref, at):
        total = ref[0, at : at + 8, :]
        for s in range(1, KV):
            total = total + ref[s, at : at + 8, :]
        return total

    query = [[rotated(total_of(qx, 16 * m + 8 * t) * ratio) for t in range(2)] for m in range(2)]
    low = lane < DH
    for h in range(HEADS):
        for m in range(2):
            x = query[m][h // 2]
            if h % 2 != m:
                x = pltpu.roll(x, DH, 1)
            qs[pl.ds(2 * h + m, 8, stride=8), :] = jnp.where(low if m == 0 else ~low, x, 0.0)

    key_head = lax.rem(lax.broadcasted_iota(jnp.int32, (16, 128), 1), HEADS)
    row_head = lax.rem(lax.broadcasted_iota(jnp.int32, (16, 128), 0), 8) // 2
    own_head = key_head == row_head
    scale = DH ** (-0.5)
    zero = jnp.zeros((8, 128), F32)
    step = 1024

    order = [lax.rem(across + 1 + t, 4) for t in range(ROWS // 2)]
    slot = 64 * (2 * lax.rem(kv, 8) + kv // 8)

    def score(t):
        rows = qs[pl.ds(pl.multiple_of(16 * order[t], 16), 16), :]
        left = jnp.concatenate(
            [
                jnp.concatenate([rows[0:8], zero], axis=1),
                jnp.concatenate([zero, rows[8:16]], axis=1),
            ],
            axis=0,
        ).astype(BF16)
        peak = jnp.full((16, 128), FLOOR, F32)
        for c in range(0, KEYS, step):
            s = jnp.dot(left, kt[order[t], :, c : c + step], preferred_element_type=F32)
            for i in range(0, step, 128):
                one = jnp.where(own_head, s[:, i : i + 128], FLOOR)
                peak = jnp.maximum(peak, one)
                sc[t % 2, :, c + i : c + i + 128] = one
        return jnp.max(peak, axis=1, keepdims=True)

    def new_token():
        everything(1, rx.at[0 : KV - 1, 0:4])
        row, share = kv // 2, lax.rem(kv, 2)
        new = total_of(rx, 0) * jnp.sum(jnp.where(sub[:, :1] == row, ratio, 0.0), axis=0, keepdims=True)
        asked = [
            jnp.sum(
                jnp.where(sub == row, jnp.where(share == 0, query[m][0], query[m][1]), 0.0), axis=0, keepdims=True
            )
            for m in range(2)
        ]
        product = jnp.where(sub == 0, asked[0], asked[1]) * rotated(new)
        wide_row = lax.broadcasted_iota(jnp.int32, (16, 128), 0)
        score_column = jnp.full((16, 1), FLOOR, F32)
        for k in range(2):
            half = jnp.sum(jnp.where(low if k == 0 else ~low, product, 0.0), axis=1, keepdims=True)
            for m in range(2):
                here = wide_row[:, :1] == 4 * along + 2 * k + m
                score_column = jnp.where(here, half[m : m + 1], score_column)
        new = new.astype(BF16).astype(F32)
        return score_column, jnp.where(lax.rem(wide_row, 4) < 2, new[2:3], new[3:4])

    stat = zero
    running = score(0)
    for t in range(ROWS // 2):
        b = 2 * order[t]
        peak = running
        if t + 1 < ROWS // 2:
            running = score(t + 1)
        else:
            own_score, own_value = new_token()
            peak = jnp.maximum(peak, own_score)
        total = jnp.zeros((16, 128), F32)
        weights = []
        for i in range(0, KEYS, 128):
            e = jnp.exp2((sc[t % 2, :, i : i + 128] - peak) * (scale * LOG2E))
            total = total + e
            weights.append(e.astype(BF16))
        total = jnp.sum(total, axis=1, keepdims=True)
        if t + 1 == ROWS // 2:
            own_weight = jnp.exp2((own_score - peak) * (scale * LOG2E))
            total = total + own_weight
        for k in range(2):
            at = 8 * (b + k)
            stat = jnp.where(lane - at == sub, peak[8 * k : 8 * k + 8] * scale, stat)
            stat = jnp.where(lane - 64 - at == sub, total[8 * k : 8 * k + 8], stat)
        if t + 1 == ROWS // 2:
            sx[pl.ds(kv, 1), :] = jnp.sum(stat, axis=0, keepdims=True)
            spread(2, lambda p: sx.at[pl.ds(kv, 1), :], sx.at[pl.ds(kv, 1), :])
        acc = jnp.zeros((16, 256), F32)
        for c in range(0, KEYS, step):
            values = jnp.concatenate([vc[b, c : c + step, :], vc[b + 1, c : c + step, :]], axis=1)
            w = jnp.concatenate(weights[c // 128 : (c + step) // 128], axis=1)
            acc = acc + jnp.dot(w, values, preferred_element_type=F32)
        acc = jnp.concatenate([acc[0:8, 0:128], acc[8:16, 128:256]], axis=0)
        if t + 1 == ROWS // 2:
            acc = acc + own_weight * own_value
        place = pl.ds(pl.multiple_of(slot + 16 * order[t], 16), 16)
        cx[place, :] = acc.astype(BF16)
        spread(3, lambda p: cx.at[place, :], cx.at[place, :])

    for copy in late_loads[:3]:
        copy.wait()
    second = jnp.zeros((8, 1), F32)
    for h in range(HEADS):
        second = jnp.where(sub[:, :1] == 2 * h, hsw[0:1, h : h + 1], second)
    gain = hg[...] * HEAD_SCALE
    square_mask = lax.rem(lax.broadcasted_iota(jnp.int32, (64, 128), 1), 64) == lax.broadcasted_iota(
        jnp.int32, (64, 128), 0
    )

    everything(2, sx.at[0 : KV - 1, :])
    stats = sx[...]
    factors = jnp.exp(stats - jnp.max(stats, axis=0, keepdims=True))
    weight_sum = jnp.sum(factors * pltpu.roll(stats, 64, 1), axis=0, keepdims=True)
    factors = factors * (1.0 / weight_sum)
    factors = jnp.where(low, factors[0:8], pltpu.roll(factors[8:16], DH, 1))
    high = factors.astype(BF16).astype(F32)
    mixing = jnp.concatenate(
        [
            jnp.concatenate(
                [jnp.where(square_mask, part[j : j + 1], 0.0).astype(BF16) for j in range(KV // 2)], axis=1
            )
            for part in (high, factors - high)
        ],
        axis=0,
    )
    everything(3, cx.at[0 : 64 * (KV - 1), :])
    both = jnp.dot(mixing, cx[...], preferred_element_type=F32)
    averaged = both[0:64] + both[64:128]
    for b in range(ROWS):
        one = averaged[8 * b : 8 * b + 8]
        difference = one - second * pltpu.roll(one, 7, 0)
        norm = lax.rsqrt(jnp.mean(difference * difference, axis=1, keepdims=True) + HEAD_EPSILON)
        df[8 * b : 8 * b + 8, :] = difference * norm * gain
    attended = jnp.concatenate([df[pl.ds(2 * h, 8, stride=8), :].astype(BF16) for h in range(HEADS)], axis=1)
    os_own[...] = jnp.dot(attended, ow_w[...], preferred_element_type=F32).astype(BF16)
    swap = pair(3, os_own, os_far)
    for copy in late_loads[3:]:
        copy.wait()
    swap.wait_recv()
    mixed = (tokens + (os_own[...].astype(F32) + os_far[...].astype(F32))).astype(BF16).astype(F32)
    mixer_scaled = (mixed * mixer_gain).astype(BF16)
    square = jnp.broadcast_to(jnp.sum(mixed * mixed, axis=1, keepdims=True), (8, 128))
    for w, ref in enumerate((gw_w, uw_w)):
        part = jnp.dot(mixer_scaled, ref[...], preferred_element_type=F32)
        for t in range(FT):
            row = (t // HT) * GR + w * HT + t % HT
            gs[pl.ds(row, 8, stride=2 * GR), :] = part[:, 128 * t : 128 * t + 128]
    high = square.astype(BF16).astype(F32)
    for half in range(2):
        gs[pl.ds(half * GR + 2 * HT, 8, stride=2 * GR), :] = high
        gs[pl.ds(half * GR + 2 * HT + 1, 8, stride=2 * GR), :] = square - high
    for j in range(KV):
        gb[j] = gs[j * GR : j * GR + GR, :].astype(BF16)
    gx[kv] = gb[kv]
    spread(5, lambda p: gb.at[p], gx.at[kv])
    everything(5, gx.at[0 : KV - 1])
    total = gx[0].astype(F32)
    for s in range(1, KV):
        total = total + gx[s].astype(F32)
    mixer_ratio = ratio_of(total[2 * HT : 2 * HT + 1] + total[2 * HT + 1 : 2 * HT + 2])
    gate = total[:HT] * mixer_ratio
    up = total[HT : 2 * HT] * mixer_ratio
    hidden = gate / (1.0 + jnp.exp(-gate)) * up
    hx[kv, 0:HT, :] = hidden.astype(BF16)
    spread(6, lambda p: hx.at[kv], hx.at[kv])
    everything(6, hx.at[0 : KV - 1])
    for s in range(KV):
        hs[16 * s : 16 * s + 16, :] = hx[s].astype(F32)
    hidden = jnp.concatenate(
        [hs[pl.ds(16 * (t // HT) + t % HT, 8, stride=32), :].astype(BF16) for t in range(FT)], axis=1
    )
    ds_own[...] = jnp.dot(hidden, dw_w[...], preferred_element_type=F32).astype(BF16)
    swap = pair(4, ds_own, ds_far)
    swap.wait_recv()
    result = mixed + (ds_own[...].astype(F32) + ds_far[...].astype(F32))
    result = jnp.where(tp == 0, result, pltpu.roll(result, DH, 1))
    out_v[...] = result[:, :64].astype(BF16)
    store = pltpu.make_async_copy(out_v, out_ref, load_sem.at[len(loads)])
    store.start()
    for copy in sends + spreads:
        copy.wait_send()
    store.wait()


def shards(
    tokens, attention_gain, query_one, query_two, key_one, key_two, value_weight, head_second_weight, head_gain,
    out_weight, mixer_gain, gate_weight, up_weight, down_weight, key_cache, value_cache,
):
    any_space = pl.BlockSpec(memory_space=pl.ANY)
    vmem = pltpu.VMEM
    dma = pltpu.SemaphoreType.DMA
    return pl.pallas_call(
        layer_kernel,
        out_shape=jax.ShapeDtypeStruct((ROWS, 64), BF16),
        in_specs=[any_space] * 17,
        out_specs=any_space,
        scratch_shapes=[
            vmem((ROWS, 64), BF16), vmem((ROWS, 64), BF16),
            vmem((1, 64), BF16), vmem((1, 64), BF16), vmem((1, 64), BF16), vmem((1, 64), BF16),
            vmem((128, 256), BF16), vmem((128, 256), BF16), vmem((128, 256), BF16), vmem((128, 256), BF16),
            vmem((128, 512), BF16), vmem((1, HEADS), F32), vmem((1, 128), F32), vmem((512, 128), BF16),
            vmem((128, FF), BF16), vmem((128, FF), BF16), vmem((FF, 128), BF16),
            vmem((ROWS, KEYS, 128), BF16), vmem((ROWS, KEYS, 128), BF16), vmem((8, 128), F32),
            vmem((256, 256), BF16), vmem((ROWS // 2, 256, KEYS), BF16),
            vmem((KV, QR, 128), F32), vmem((KV * 8, 128), F32), vmem((KV, 8, 128), F32),
            vmem((KV * 64, 128), BF16), vmem((KV, 128), F32),
            vmem((KV * GR, 128), F32), vmem((KV, GR, 128), BF16), vmem((KV, GR, 128), BF16),
            vmem((KV, 16, 128), BF16), vmem((KV * 16, 128), F32), vmem((64, 128), F32),
            vmem((2, 16, KEYS), F32), vmem((64, 128), F32),
            vmem((8, 128), BF16), vmem((8, 128), BF16), vmem((8, 128), BF16), vmem((8, 128), BF16), vmem((ROWS, 64), BF16),
            dma((18,)), dma((5,)), dma((5,)), dma((7,)), dma((7,)),
        ],
        compiler_params=pltpu.CompilerParams(
            collective_id=0, has_side_effects=True, vmem_limit_bytes=60 * 1024 * 1024
        ),
        name="layer",
    )(
        tokens, attention_gain.reshape(1, -1), query_one, query_two, key_one, key_two, value_weight,
        head_second_weight.reshape(1, -1), head_gain.reshape(1, -1), out_weight, mixer_gain.reshape(1, -1),
        gate_weight, up_weight, down_weight,
        key_cache.reshape(ROWS, KEYS, 128), value_cache.reshape(ROWS, KEYS, 128), jnp.asarray(rotary_tables()),
    )


def solution(mesh):
    both = ("kv", "tp")
    return jax.shard_map(
        shards,
        mesh=mesh,
        in_specs=(
            P("dp", both), P(both), P("kv", "tp"), P("kv", "tp"), P("kv", "tp"), P("kv", "tp"), P("kv", "tp"),
            P("tp"), P(), P("tp", "kv"), P(both), P("kv", "tp"), P("kv", "tp"), P("tp", "kv"),
            P("dp", "kv", "tp", None), P("dp", "kv", "tp", None),
        ),
        out_specs=P("dp", both),
        check_vma=False,
    )
```

```python
import jax
import jax.numpy as jnp
import numpy as np
from jax import lax
from jax.experimental import pallas as pl
from jax.experimental.pallas import tpu as pltpu
from jax.sharding import PartitionSpec as P

MESH = pl.DeviceIdType.MESH
F32 = jnp.float32
BF16 = jnp.bfloat16

D = 2048
DH = 64
POSITIONS = 1024
HEADS = 4
ROWS = 8
KV = 16
FF = 2816
FT = FF // 128
HT = FT // 2
CACHE = KV * POSITIONS
NORM_EPSILON = 1e-06
HEAD_EPSILON = 1e-05
HEAD_SCALE = 0.8
FLOOR = -1e30
LOG2E = 1.4426950408889634
KEYS = POSITIONS * HEADS
QR = 33
GR = 24


OFFSETS = sorted(
    ((i, j) for i in range(4) for j in range(4) if (i, j) != (0, 0)),
    key=lambda o: -min(o[0], 4 - o[0]) - min(o[1], 4 - o[1]),
)


def rotary_tables():
    half = DH // 2
    index = np.arange(half, dtype=np.float32) / np.float32(half)
    frequency = (np.float32(1.0) / np.power(np.float32(10000.0), index)).astype(np.float32)
    angle = (np.float32(CACHE) * frequency).astype(np.float32).astype(np.float64)
    cosine = np.tile(np.cos(angle).astype(np.float32), 4)
    sine = np.sin(angle).astype(np.float32)
    sine = np.tile(np.concatenate([-sine, sine]), 2)
    table = np.zeros((8, 128), np.float32)
    table[0], table[1] = cosine, sine
    return table


def layer_kernel(
    tok_h, ag_h, q1_h, q2_h, k1_h, k2_h, vw_h, hsw_h, hg_h, ow_h, mg_h, gw_h, uw_h, dw_h, kc_h, vc_h, tab_h,
    out_ref,
    tok_own, tok_far, ag_own, ag_far, mg_own, mg_far,
    q1_w, q2_w, k1_w, k2_w, vw_w, hsw, hg, ow_w, gw_w, uw_w, dw_w, kc, vc, tab,
    unit, kt, qx, rs, rx, cx, sx, gs, gb, gx, hx, hs, qs, sc, df, os_own, os_far, dw_far, ds, out_v,
    load_sem, pair_send, pair_recv, all_send, all_recv,
):
    dp, kv, tp = (lax.axis_index(a) for a in ("dp", "kv", "tp"))
    barrier = pltpu.get_barrier_semaphore()
    partner = (dp, kv, 1 - tp)
    across, along = kv // 4, lax.rem(kv, 4)
    peers = [lax.rem(across + i, 4) * 4 + lax.rem(along + j, 4) for i, j in OFFSETS]
    for p in peers:
        pl.semaphore_signal(barrier, 1, device_id=(dp, p, tp), device_id_type=MESH)
    pl.semaphore_signal(barrier, 1, device_id=partner, device_id_type=MESH)

    loads = []

    def load(src, dst):
        copy = pltpu.make_async_copy(src, dst, load_sem.at[len(loads)])
        copy.start()
        loads.append(copy)
        return copy

    first = [load(a, b) for a, b in ((tok_h, tok_own), (ag_h, ag_own), (mg_h, mg_own))]
    q_loads = [load(a, b) for a, b in ((q1_h, q1_w), (q2_h, q2_w), (tab_h, tab))]
    down_load = load(dw_h, dw_w)
    kv_loads = [load(a, b) for a, b in ((k1_h, k1_w), (k2_h, k2_w), (vw_h, vw_w))]
    cache_loads = [load(kc_h, kc), load(vc_h, vc)]
    late_loads = [
        load(a, b)
        for a, b in ((hsw_h, hsw), (hg_h, hg), (ow_h, ow_w), (gw_h, gw_w), (uw_h, uw_w))
    ]
    for copy in first:
        copy.wait()
    pl.semaphore_wait(barrier, KV)

    sends, spreads = [], []

    def pair(k, src, dst):
        copy = pltpu.make_async_remote_copy(
            src, dst, pair_send.at[k], pair_recv.at[k], device_id=partner, device_id_type=MESH
        )
        copy.start()
        sends.append(copy)
        return copy

    def spread(stage, source, target):
        for p in peers:
            pltpu.make_async_remote_copy(
                source(p), target, all_send.at[stage], all_recv.at[stage],
                device_id=(dp, p, tp), device_id_type=MESH,
            ).start()

    def everything(stage, most):
        copy = pltpu.make_async_remote_copy(
            most, most, all_send.at[stage], all_recv.at[stage], device_id=partner, device_id_type=MESH
        )
        spreads.append(copy)
        copy.wait_recv()

    swaps = [pair(0, tok_own, tok_far), pair(1, ag_own, ag_far), pair(2, mg_own, mg_far)]
    lane = lax.broadcasted_iota(jnp.int32, (8, 128), 1)
    sub = lax.broadcasted_iota(jnp.int32, (8, 128), 0)
    diagonal = lane == sub
    for copy in q_loads:
        copy.wait()
    down_load.wait()
    swap_down = pair(4, dw_w, dw_far)
    for copy in swaps:
        copy.wait_recv()

    def joined(own, far):
        own, far = own[...].astype(F32), far[...].astype(F32)
        return jnp.concatenate([jnp.where(tp == 0, own, far), jnp.where(tp == 0, far, own)], axis=-1)

    tokens = joined(tok_own, tok_far)
    scaled = (tokens * joined(ag_own, ag_far)).astype(BF16)
    mixer_gain = joined(mg_own, mg_far)
    square = jnp.sum(tokens * tokens, axis=1, keepdims=True)
    square_row = jnp.sum(jnp.where(diagonal, square, 0.0), axis=0, keepdims=True)
    for w, ref in enumerate((q1_w, q2_w)):
        part = jnp.dot(scaled, ref[...], preferred_element_type=F32)
        for t in range(2):
            qx[kv, 16 * w + 8 * t : 16 * w + 8 * t + 8, :] = part[:, 128 * t : 128 * t + 128]
    qx[kv, 32:33, :] = square_row
    spread(0, lambda p: qx.at[kv], qx.at[kv])

    for copy in kv_loads:
        copy.wait()
    for w, ref in enumerate((k1_w, k2_w)):
        part = jnp.dot(scaled, ref[...], preferred_element_type=F32)
        for t in range(2):
            rs[pl.ds(8 * t + w, 8, stride=16), :] = part[:, 128 * t : 128 * t + 128]
    part = jnp.dot(scaled, vw_w[...], preferred_element_type=F32)
    for t in range(HEADS):
        rs[pl.ds(8 * (t // 2) + 2 + t % 2, 8, stride=16), :] = part[:, 128 * t : 128 * t + 128]
    rx[kv] = rs[pl.ds(pl.multiple_of(8 * kv, 8), 8), :]
    spread(1, lambda p: rs.at[pl.ds(pl.multiple_of(8 * p, 8), 4), :], rx.at[kv, 0:4])

    wide = (256, 256)
    unit[...] = (lax.broadcasted_iota(jnp.int32, wide, 0) == lax.broadcasted_iota(jnp.int32, wide, 1)).astype(BF16)
    cache_loads[0].wait()

    def turn(c, carry):
        at = pl.multiple_of(c * 512, 512)
        for b in range(0, ROWS, 2):
            keys = jnp.concatenate([kc[b, pl.ds(at, 512), :], kc[b + 1, pl.ds(at, 512), :]], axis=1)
            turned = lax.dot_general(unit[...], keys, (((1,), (1,)), ((), ())), preferred_element_type=F32)
            kt[b // 2, :, pl.ds(at, 512)] = turned.astype(BF16)
        return carry

    lax.fori_loop(0, KEYS // 512, turn, 0)
    cache_loads[1].wait()
    everything(0, qx.at[0 : KV - 1])

    def ratio_of(total):
        return lax.rsqrt(total / D + NORM_EPSILON)

    square_total = qx[0, 32:33, :]
    for s in range(1, KV):
        square_total = square_total + qx[s, 32:33, :]
    ratio_row = ratio_of(square_total)
    ratio = jnp.sum(jnp.where(diagonal, ratio_row, 0.0), axis=1, keepdims=True)
    cosine, sine = tab[0:1, :], tab[1:2, :]
    lead = lax.rem(lane, DH) < DH // 2

    def rotated(x):
        turned = jnp.where(lead, pltpu.roll(x, 128 - DH // 2, 1), pltpu.roll(x, DH // 2, 1))
        return (x * cosine + turned * sine).astype(BF16).astype(F32)

    def total_of(ref, at):
        total = ref[0, at : at + 8, :]
        for s in range(1, KV):
            total = total + ref[s, at : at + 8, :]
        return total

    query = [[rotated(total_of(qx, 16 * m + 8 * t) * ratio) for t in range(2)] for m in range(2)]
    low = lane < DH
    for h in range(HEADS):
        for m in range(2):
            x = query[m][h // 2]
            if h % 2 != m:
                x = pltpu.roll(x, DH, 1)
            qs[pl.ds(2 * h + m, 8, stride=8), :] = jnp.where(low if m == 0 else ~low, x, 0.0)

    key_head = lax.rem(lax.broadcasted_iota(jnp.int32, (16, 128), 1), HEADS)
    row_head = lax.rem(lax.broadcasted_iota(jnp.int32, (16, 128), 0), 8) // 2
    own_head = key_head == row_head
    scale = DH ** (-0.5)
    zero = jnp.zeros((8, 128), F32)
    step = 1024

    order = [lax.rem(across + 1 + t, 4) for t in range(ROWS // 2)]
    slot = 64 * (2 * lax.rem(kv, 8) + kv // 8)

    def score(t):
        rows = qs[pl.ds(pl.multiple_of(16 * order[t], 16), 16), :]
        left = jnp.concatenate(
            [
                jnp.concatenate([rows[0:8], zero], axis=1),
                jnp.concatenate([zero, rows[8:16]], axis=1),
            ],
            axis=0,
        ).astype(BF16)
        peak = jnp.full((16, 128), FLOOR, F32)
        for c in range(0, KEYS, step):
            s = jnp.dot(left, kt[order[t], :, c : c + step], preferred_element_type=F32)
            for i in range(0, step, 128):
                one = jnp.where(own_head, s[:, i : i + 128], FLOOR)
                peak = jnp.maximum(peak, one)
                sc[t % 2, :, c + i : c + i + 128] = one
        return jnp.max(peak, axis=1, keepdims=True)

    def new_token():
        everything(1, rx.at[0 : KV - 1, 0:4])
        row, share = kv // 2, lax.rem(kv, 2)
        new = total_of(rx, 0) * jnp.sum(jnp.where(sub[:, :1] == row, ratio, 0.0), axis=0, keepdims=True)
        asked = [
            jnp.sum(
                jnp.where(sub == row, jnp.where(share == 0, query[m][0], query[m][1]), 0.0), axis=0, keepdims=True
            )
            for m in range(2)
        ]
        product = jnp.where(sub == 0, asked[0], asked[1]) * rotated(new)
        wide_row = lax.broadcasted_iota(jnp.int32, (16, 128), 0)
        score_column = jnp.full((16, 1), FLOOR, F32)
        for k in range(2):
            half = jnp.sum(jnp.where(low if k == 0 else ~low, product, 0.0), axis=1, keepdims=True)
            for m in range(2):
                here = wide_row[:, :1] == 4 * along + 2 * k + m
                score_column = jnp.where(here, half[m : m + 1], score_column)
        new = new.astype(BF16).astype(F32)
        return score_column, jnp.where(lax.rem(wide_row, 4) < 2, new[2:3], new[3:4])

    stat = zero
    running = score(0)
    for t in range(ROWS // 2):
        b = 2 * order[t]
        peak = running
        if t + 1 < ROWS // 2:
            running = score(t + 1)
        else:
            own_score, own_value = new_token()
            peak = jnp.maximum(peak, own_score)
        total = jnp.zeros((16, 128), F32)
        weights = []
        for i in range(0, KEYS, 128):
            e = jnp.exp2((sc[t % 2, :, i : i + 128] - peak) * (scale * LOG2E))
            total = total + e
            weights.append(e.astype(BF16))
        total = jnp.sum(total, axis=1, keepdims=True)
        if t + 1 == ROWS // 2:
            own_weight = jnp.exp2((own_score - peak) * (scale * LOG2E))
            total = total + own_weight
        for k in range(2):
            at = 8 * (b + k)
            stat = jnp.where(lane - at == sub, peak[8 * k : 8 * k + 8] * scale, stat)
            stat = jnp.where(lane - 64 - at == sub, total[8 * k : 8 * k + 8], stat)
        if t + 1 == ROWS // 2:
            sx[pl.ds(kv, 1), :] = jnp.sum(stat, axis=0, keepdims=True)
            spread(2, lambda p: sx.at[pl.ds(kv, 1), :], sx.at[pl.ds(kv, 1), :])
        acc = jnp.zeros((16, 256), F32)
        for c in range(0, KEYS, step):
            values = jnp.concatenate([vc[b, c : c + step, :], vc[b + 1, c : c + step, :]], axis=1)
            w = jnp.concatenate(weights[c // 128 : (c + step) // 128], axis=1)
            acc = acc + jnp.dot(w, values, preferred_element_type=F32)
        acc = jnp.concatenate([acc[0:8, 0:128], acc[8:16, 128:256]], axis=0)
        if t + 1 == ROWS // 2:
            acc = acc + own_weight * own_value
        place = pl.ds(pl.multiple_of(slot + 16 * order[t], 16), 16)
        cx[place, :] = acc.astype(BF16)
        spread(3, lambda p: cx.at[place, :], cx.at[place, :])

    for copy in late_loads[:3]:
        copy.wait()
    second = jnp.zeros((8, 1), F32)
    for h in range(HEADS):
        second = jnp.where(sub[:, :1] == 2 * h, hsw[0:1, h : h + 1], second)
    gain = hg[...] * HEAD_SCALE
    square_mask = lax.rem(lax.broadcasted_iota(jnp.int32, (64, 128), 1), 64) == lax.broadcasted_iota(
        jnp.int32, (64, 128), 0
    )

    everything(2, sx.at[0 : KV - 1, :])
    stats = sx[...]
    factors = jnp.exp(stats - jnp.max(stats, axis=0, keepdims=True))
    weight_sum = jnp.sum(factors * pltpu.roll(stats, 64, 1), axis=0, keepdims=True)
    factors = factors * (1.0 / weight_sum)
    factors = jnp.where(low, factors[0:8], pltpu.roll(factors[8:16], DH, 1))
    high = factors.astype(BF16).astype(F32)
    mixing = jnp.concatenate(
        [
            jnp.concatenate(
                [jnp.where(square_mask, part[j : j + 1], 0.0).astype(BF16) for j in range(KV // 2)], axis=1
            )
            for part in (high, factors - high)
        ],
        axis=0,
    )
    everything(3, cx.at[0 : 64 * (KV - 1), :])
    both = jnp.dot(mixing, cx[...], preferred_element_type=F32)
    averaged = both[0:64] + both[64:128]
    for b in range(ROWS):
        one = averaged[8 * b : 8 * b + 8]
        difference = one - second * pltpu.roll(one, 7, 0)
        norm = lax.rsqrt(jnp.mean(difference * difference, axis=1, keepdims=True) + HEAD_EPSILON)
        df[8 * b : 8 * b + 8, :] = difference * norm * gain
    attended = jnp.concatenate([df[pl.ds(2 * h, 8, stride=8), :].astype(BF16) for h in range(HEADS)], axis=1)
    os_own[...] = jnp.dot(attended, ow_w[...], preferred_element_type=F32).astype(BF16)
    swap = pair(3, os_own, os_far)
    for copy in late_loads[3:]:
        copy.wait()
    swap.wait_recv()
    mixed = (tokens + (os_own[...].astype(F32) + os_far[...].astype(F32))).astype(BF16).astype(F32)
    mixer_scaled = (mixed * mixer_gain).astype(BF16)
    square = jnp.broadcast_to(jnp.sum(mixed * mixed, axis=1, keepdims=True), (8, 128))
    for w, ref in enumerate((gw_w, uw_w)):
        part = jnp.dot(mixer_scaled, ref[...], preferred_element_type=F32)
        for t in range(FT):
            row = (t // HT) * GR + w * HT + t % HT
            gs[pl.ds(row, 8, stride=2 * GR), :] = part[:, 128 * t : 128 * t + 128]
    high = square.astype(BF16).astype(F32)
    for half in range(2):
        gs[pl.ds(half * GR + 2 * HT, 8, stride=2 * GR), :] = high
        gs[pl.ds(half * GR + 2 * HT + 1, 8, stride=2 * GR), :] = square - high
    for j in range(KV):
        gb[j] = gs[j * GR : j * GR + GR, :].astype(BF16)
    gx[kv] = gb[kv]
    spread(5, lambda p: gb.at[p], gx.at[kv])
    everything(5, gx.at[0 : KV - 1])
    total = gx[0].astype(F32)
    for s in range(1, KV):
        total = total + gx[s].astype(F32)
    mixer_ratio = ratio_of(total[2 * HT : 2 * HT + 1] + total[2 * HT + 1 : 2 * HT + 2])
    gate = total[:HT] * mixer_ratio
    up = total[HT : 2 * HT] * mixer_ratio
    hidden = gate / (1.0 + jnp.exp(-gate)) * up
    mine = hx.at[KV * tp + kv, 0 : HT + 1]
    hx[KV * tp + kv, 0 : HT + 1, :] = jnp.concatenate([hidden, zero[0:1]], axis=0).astype(BF16)

    def share(p, core):
        pltpu.make_async_remote_copy(
            mine, mine, all_send.at[6], all_recv.at[6], device_id=(dp, p, core), device_id_type=MESH
        ).start()

    for p in peers:
        share(p, 1 - tp)
        share(p, tp)
    share(kv, 1 - tp)
    swap_down.wait_recv()
    everything(6, hx.at[0 : 2 * KV - 1, 0 : HT + 1])
    for s in range(2 * KV):
        hs[16 * s : 16 * s + 16, :] = hx[s].astype(F32)
    result = zero
    for core, weights in ((tp, dw_w), (1 - tp, dw_far)):
        at = pl.multiple_of(16 * KV * core, 8)
        hidden = jnp.concatenate(
            [
                jnp.concatenate([hs[pl.ds(at + 128 * k + t, 8, stride=16), :] for k in range(2)], axis=0).astype(BF16)
                for t in range(HT)
            ],
            axis=1,
        )
        down = jnp.concatenate([weights[0 : FF // 2, :], weights[FF // 2 : FF, :]], axis=1)
        part = jnp.dot(hidden, down, preferred_element_type=F32)
        ds[0:16, :] = part[:, 0:128]
        ds[16:32, :] = part[:, 128:256]
        part = ds[pl.ds(0, 8, stride=2), :] + ds[pl.ds(17, 8, stride=2), :]
        result = result + part.astype(BF16).astype(F32)
    result = mixed + result
    result = jnp.where(tp == 0, result, pltpu.roll(result, DH, 1))
    out_v[...] = result[:, :64].astype(BF16)
    store = pltpu.make_async_copy(out_v, out_ref, load_sem.at[len(loads)])
    store.start()
    for copy in sends + spreads:
        copy.wait_send()
    store.wait()


def shards(
    tokens, attention_gain, query_one, query_two, key_one, key_two, value_weight, head_second_weight, head_gain,
    out_weight, mixer_gain, gate_weight, up_weight, down_weight, key_cache, value_cache,
):
    any_space = pl.BlockSpec(memory_space=pl.ANY)
    vmem = pltpu.VMEM
    dma = pltpu.SemaphoreType.DMA
    return pl.pallas_call(
        layer_kernel,
        out_shape=jax.ShapeDtypeStruct((ROWS, 64), BF16),
        in_specs=[any_space] * 17,
        out_specs=any_space,
        scratch_shapes=[
            vmem((ROWS, 64), BF16), vmem((ROWS, 64), BF16),
            vmem((1, 64), BF16), vmem((1, 64), BF16), vmem((1, 64), BF16), vmem((1, 64), BF16),
            vmem((128, 256), BF16), vmem((128, 256), BF16), vmem((128, 256), BF16), vmem((128, 256), BF16),
            vmem((128, 512), BF16), vmem((1, HEADS), F32), vmem((1, 128), F32), vmem((512, 128), BF16),
            vmem((128, FF), BF16), vmem((128, FF), BF16), vmem((FF, 128), BF16),
            vmem((ROWS, KEYS, 128), BF16), vmem((ROWS, KEYS, 128), BF16), vmem((8, 128), F32),
            vmem((256, 256), BF16), vmem((ROWS // 2, 256, KEYS), BF16),
            vmem((KV, QR, 128), F32), vmem((KV * 8, 128), F32), vmem((KV, 8, 128), F32),
            vmem((KV * 64, 128), BF16), vmem((KV, 128), F32),
            vmem((KV * GR, 128), F32), vmem((KV, GR, 128), BF16), vmem((KV, GR, 128), BF16),
            vmem((2 * KV, 16, 128), BF16), vmem((2 * KV * 16, 128), F32), vmem((64, 128), F32),
            vmem((2, 16, KEYS), F32), vmem((64, 128), F32),
            vmem((8, 128), BF16), vmem((8, 128), BF16), vmem((FF, 128), BF16), vmem((32, 128), F32), vmem((ROWS, 64), BF16),
            dma((18,)), dma((5,)), dma((5,)), dma((7,)), dma((7,)),
        ],
        compiler_params=pltpu.CompilerParams(
            collective_id=0, has_side_effects=True, vmem_limit_bytes=60 * 1024 * 1024
        ),
        name="layer",
    )(
        tokens, attention_gain.reshape(1, -1), query_one, query_two, key_one, key_two, value_weight,
        head_second_weight.reshape(1, -1), head_gain.reshape(1, -1), out_weight, mixer_gain.reshape(1, -1),
        gate_weight, up_weight, down_weight,
        key_cache.reshape(ROWS, KEYS, 128), value_cache.reshape(ROWS, KEYS, 128), jnp.asarray(rotary_tables()),
    )


def solution(mesh):
    both = ("kv", "tp")
    return jax.shard_map(
        shards,
        mesh=mesh,
        in_specs=(
            P("dp", both), P(both), P("kv", "tp"), P("kv", "tp"), P("kv", "tp"), P("kv", "tp"), P("kv", "tp"),
            P("tp"), P(), P("tp", "kv"), P(both), P("kv", "tp"), P("kv", "tp"), P("tp", "kv"),
            P("dp", "kv", "tp", None), P("dp", "kv", "tp", None),
        ),
        out_specs=P("dp", both),
        check_vma=False,
    )
```

```python
import jax
import jax.numpy as jnp
import numpy as np
from jax import lax
from jax.experimental import pallas as pl
from jax.experimental.pallas import tpu as pltpu
from jax.sharding import PartitionSpec as P

MESH = pl.DeviceIdType.MESH
F32 = jnp.float32
BF16 = jnp.bfloat16

D = 2048
DH = 64
POSITIONS = 1024
HEADS = 4
ROWS = 8
KV = 16
FF = 2816
FT = FF // 128
HT = FT // 2
CACHE = KV * POSITIONS
NORM_EPSILON = 1e-06
HEAD_EPSILON = 1e-05
HEAD_SCALE = 0.8
FLOOR = -1e30
LOG2E = 1.4426950408889634
KEYS = POSITIONS * HEADS
QR = 33
GR = 24


OFFSETS = sorted(
    ((i, j) for i in range(4) for j in range(4) if (i, j) != (0, 0)),
    key=lambda o: -min(o[0], 4 - o[0]) - min(o[1], 4 - o[1]),
)


def rotary_tables():
    half = DH // 2
    index = np.arange(half, dtype=np.float32) / np.float32(half)
    frequency = (np.float32(1.0) / np.power(np.float32(10000.0), index)).astype(np.float32)
    angle = (np.float32(CACHE) * frequency).astype(np.float32).astype(np.float64)
    cosine = np.tile(np.cos(angle).astype(np.float32), 4)
    sine = np.sin(angle).astype(np.float32)
    sine = np.tile(np.concatenate([-sine, sine]), 2)
    table = np.zeros((8, 128), np.float32)
    table[0], table[1] = cosine, sine
    return table


def layer_kernel(
    tok_h, ag_h, q1_h, q2_h, k1_h, k2_h, vw_h, hsw_h, hg_h, ow_h, mg_h, gw_h, uw_h, dw_h, kc_h, vc_h, tab_h,
    out_ref,
    tok_own, tok_far, ag_own, ag_far, mg_own, mg_far,
    q1_w, q2_w, k1_w, k2_w, vw_w, hsw, hg, ow_w, gw_w, uw_w, dw_w, kc, vc, tab,
    unit, kt, qx, rs, rx, cx, sx, gs, gb, gx, hx, hs, qs, sc, df, os_own, os_far, dw_far, ds, out_v,
    ready, load_sem, pair_send, pair_recv, all_send, all_recv,
):
    dp, kv, tp = (lax.axis_index(a) for a in ("dp", "kv", "tp"))
    barrier = pltpu.get_barrier_semaphore()
    partner = (dp, kv, 1 - tp)
    across, along = kv // 4, lax.rem(kv, 4)
    peers = [lax.rem(across + i, 4) * 4 + lax.rem(along + j, 4) for i, j in OFFSETS]
    for p in peers:
        pl.semaphore_signal(barrier, 1, device_id=(dp, p, 1), device_id_type=MESH)
    pl.semaphore_signal(barrier, 1, device_id=partner, device_id_type=MESH)

    loads = []

    def load(src, dst):
        copy = pltpu.make_async_copy(src, dst, load_sem.at[len(loads)])
        copy.start()
        loads.append(copy)
        return copy

    first = [load(a, b) for a, b in ((tok_h, tok_own), (ag_h, ag_own), (mg_h, mg_own))]
    q_loads = [load(a, b) for a, b in ((q1_h, q1_w), (q2_h, q2_w), (tab_h, tab))]
    down_load = load(dw_h, dw_w)
    kv_loads = [load(a, b) for a, b in ((k1_h, k1_w), (k2_h, k2_w), (vw_h, vw_w))]
    cache_loads = [load(kc_h, kc), load(vc_h, vc)]
    late_loads = [
        load(a, b)
        for a, b in ((hsw_h, hsw), (hg_h, hg), (ow_h, ow_w), (gw_h, gw_w), (uw_h, uw_w))
    ]
    @pl.when(tp == 0)
    def _():
        pl.semaphore_wait(barrier, 1)
        pl.semaphore_signal(ready.at[0], 1, device_id=partner, device_id_type=MESH)

    @pl.when(tp == 1)
    def _():
        pl.semaphore_wait(ready.at[0], 1)

    for copy in first:
        copy.wait()

    sends, spreads = [], []

    def pair(k, src, dst):
        copy = pltpu.make_async_remote_copy(
            src, dst, pair_send.at[k], pair_recv.at[k], device_id=partner, device_id_type=MESH
        )
        copy.start()
        sends.append(copy)
        return copy

    def spread(stage, source, target):
        for p in peers:
            pltpu.make_async_remote_copy(
                source(p), target, all_send.at[stage], all_recv.at[stage],
                device_id=(dp, p, tp), device_id_type=MESH,
            ).start()

    def everything(stage, most):
        copy = pltpu.make_async_remote_copy(
            most, most, all_send.at[stage], all_recv.at[stage], device_id=partner, device_id_type=MESH
        )
        spreads.append(copy)
        copy.wait_recv()

    swaps = [pair(0, tok_own, tok_far), pair(1, ag_own, ag_far), pair(2, mg_own, mg_far)]
    lane = lax.broadcasted_iota(jnp.int32, (8, 128), 1)
    sub = lax.broadcasted_iota(jnp.int32, (8, 128), 0)
    diagonal = lane == sub
    for copy in q_loads:
        copy.wait()
    down_load.wait()
    swap_down = pair(4, dw_w, dw_far)
    for copy in swaps:
        copy.wait_recv()

    def joined(own, far):
        own, far = own[...].astype(F32), far[...].astype(F32)
        return jnp.concatenate([jnp.where(tp == 0, own, far), jnp.where(tp == 0, far, own)], axis=-1)

    tokens = joined(tok_own, tok_far)
    scaled = (tokens * joined(ag_own, ag_far)).astype(BF16)
    mixer_gain = joined(mg_own, mg_far)
    square = jnp.sum(tokens * tokens, axis=1, keepdims=True)
    square_row = jnp.sum(jnp.where(diagonal, square, 0.0), axis=0, keepdims=True)
    for w, ref in enumerate((q1_w, q2_w)):
        part = jnp.dot(scaled, ref[...], preferred_element_type=F32)
        for t in range(2):
            qx[kv, 16 * w + 8 * t : 16 * w + 8 * t + 8, :] = part[:, 128 * t : 128 * t + 128]
    qx[kv, 32:33, :] = square_row
    for copy in kv_loads:
        copy.wait()
    for w, ref in enumerate((k1_w, k2_w)):
        part = jnp.dot(scaled, ref[...], preferred_element_type=F32)
        for t in range(2):
            rs[pl.ds(8 * t + w, 8, stride=16), :] = part[:, 128 * t : 128 * t + 128]
    part = jnp.dot(scaled, vw_w[...], preferred_element_type=F32)
    for t in range(HEADS):
        rs[pl.ds(8 * (t // 2) + 2 + t % 2, 8, stride=16), :] = part[:, 128 * t : 128 * t + 128]
    @pl.when(tp == 1)
    def _():
        pl.semaphore_wait(barrier, 2 * KV - 1)
        pl.semaphore_signal(ready.at[1], 1, device_id=partner, device_id_type=MESH)

    @pl.when(tp == 0)
    def _():
        pl.semaphore_wait(ready.at[1], 1)

    spread(0, lambda p: qx.at[kv], qx.at[kv])
    rx[kv] = rs[pl.ds(pl.multiple_of(8 * kv, 8), 8), :]
    spread(1, lambda p: rs.at[pl.ds(pl.multiple_of(8 * p, 8), 4), :], rx.at[kv, 0:4])

    wide = (256, 256)
    unit[...] = (lax.broadcasted_iota(jnp.int32, wide, 0) == lax.broadcasted_iota(jnp.int32, wide, 1)).astype(BF16)
    cache_loads[0].wait()

    def turn(c, carry):
        at = pl.multiple_of(c * 512, 512)
        for b in range(0, ROWS, 2):
            keys = jnp.concatenate([kc[b, pl.ds(at, 512), :], kc[b + 1, pl.ds(at, 512), :]], axis=1)
            turned = lax.dot_general(unit[...], keys, (((1,), (1,)), ((), ())), preferred_element_type=F32)
            kt[b // 2, :, pl.ds(at, 512)] = turned.astype(BF16)
        return carry

    lax.fori_loop(0, KEYS // 512, turn, 0)
    cache_loads[1].wait()
    everything(0, qx.at[0 : KV - 1])

    def ratio_of(total):
        return lax.rsqrt(total / D + NORM_EPSILON)

    square_total = qx[0, 32:33, :]
    for s in range(1, KV):
        square_total = square_total + qx[s, 32:33, :]
    ratio_row = ratio_of(square_total)
    ratio = jnp.sum(jnp.where(diagonal, ratio_row, 0.0), axis=1, keepdims=True)
    cosine, sine = tab[0:1, :], tab[1:2, :]
    lead = lax.rem(lane, DH) < DH // 2

    def rotated(x):
        turned = jnp.where(lead, pltpu.roll(x, 128 - DH // 2, 1), pltpu.roll(x, DH // 2, 1))
        return (x * cosine + turned * sine).astype(BF16).astype(F32)

    def total_of(ref, at):
        total = ref[0, at : at + 8, :]
        for s in range(1, KV):
            total = total + ref[s, at : at + 8, :]
        return total

    query = [[rotated(total_of(qx, 16 * m + 8 * t) * ratio) for t in range(2)] for m in range(2)]
    low = lane < DH
    for h in range(HEADS):
        for m in range(2):
            x = query[m][h // 2]
            if h % 2 != m:
                x = pltpu.roll(x, DH, 1)
            qs[pl.ds(2 * h + m, 8, stride=8), :] = jnp.where(low if m == 0 else ~low, x, 0.0)

    key_head = lax.rem(lax.broadcasted_iota(jnp.int32, (16, 128), 1), HEADS)
    row_head = lax.rem(lax.broadcasted_iota(jnp.int32, (16, 128), 0), 8) // 2
    own_head = key_head == row_head
    scale = DH ** (-0.5)
    zero = jnp.zeros((8, 128), F32)
    step = 1024

    order = [lax.rem(across + 1 + t, 4) for t in range(ROWS // 2)]
    slot = 64 * (2 * lax.rem(kv, 8) + kv // 8)

    def score(t):
        rows = qs[pl.ds(pl.multiple_of(16 * order[t], 16), 16), :]
        left = jnp.concatenate(
            [
                jnp.concatenate([rows[0:8], zero], axis=1),
                jnp.concatenate([zero, rows[8:16]], axis=1),
            ],
            axis=0,
        ).astype(BF16)
        peak = jnp.full((16, 128), FLOOR, F32)
        for c in range(0, KEYS, step):
            s = jnp.dot(left, kt[order[t], :, c : c + step], preferred_element_type=F32)
            for i in range(0, step, 128):
                one = jnp.where(own_head, s[:, i : i + 128], FLOOR)
                peak = jnp.maximum(peak, one)
                sc[t % 2, :, c + i : c + i + 128] = one
        return jnp.max(peak, axis=1, keepdims=True)

    def new_token():
        everything(1, rx.at[0 : KV - 1, 0:4])
        row, share = kv // 2, lax.rem(kv, 2)
        new = total_of(rx, 0) * jnp.sum(jnp.where(sub[:, :1] == row, ratio, 0.0), axis=0, keepdims=True)
        asked = [
            jnp.sum(
                jnp.where(sub == row, jnp.where(share == 0, query[m][0], query[m][1]), 0.0), axis=0, keepdims=True
            )
            for m in range(2)
        ]
        product = jnp.where(sub == 0, asked[0], asked[1]) * rotated(new)
        wide_row = lax.broadcasted_iota(jnp.int32, (16, 128), 0)
        score_column = jnp.full((16, 1), FLOOR, F32)
        for k in range(2):
            half = jnp.sum(jnp.where(low if k == 0 else ~low, product, 0.0), axis=1, keepdims=True)
            for m in range(2):
                here = wide_row[:, :1] == 4 * along + 2 * k + m
                score_column = jnp.where(here, half[m : m + 1], score_column)
        new = new.astype(BF16).astype(F32)
        return score_column, jnp.where(lax.rem(wide_row, 4) < 2, new[2:3], new[3:4])

    stat = zero
    running = score(0)
    for t in range(ROWS // 2):
        b = 2 * order[t]
        peak = running
        if t + 1 < ROWS // 2:
            running = score(t + 1)
        else:
            own_score, own_value = new_token()
            peak = jnp.maximum(peak, own_score)
        total = jnp.zeros((16, 128), F32)
        weights = []
        for i in range(0, KEYS, 128):
            e = jnp.exp2((sc[t % 2, :, i : i + 128] - peak) * (scale * LOG2E))
            total = total + e
            weights.append(e.astype(BF16))
        total = jnp.sum(total, axis=1, keepdims=True)
        if t + 1 == ROWS // 2:
            own_weight = jnp.exp2((own_score - peak) * (scale * LOG2E))
            total = total + own_weight
        for k in range(2):
            at = 8 * (b + k)
            stat = jnp.where(lane - at == sub, peak[8 * k : 8 * k + 8] * scale, stat)
            stat = jnp.where(lane - 64 - at == sub, total[8 * k : 8 * k + 8], stat)
        if t + 1 == ROWS // 2:
            sx[pl.ds(kv, 1), :] = jnp.sum(stat, axis=0, keepdims=True)
            spread(2, lambda p: sx.at[pl.ds(kv, 1), :], sx.at[pl.ds(kv, 1), :])
        acc = jnp.zeros((16, 256), F32)
        for c in range(0, KEYS, step):
            values = jnp.concatenate([vc[b, c : c + step, :], vc[b + 1, c : c + step, :]], axis=1)
            w = jnp.concatenate(weights[c // 128 : (c + step) // 128], axis=1)
            acc = acc + jnp.dot(w, values, preferred_element_type=F32)
        acc = jnp.concatenate([acc[0:8, 0:128], acc[8:16, 128:256]], axis=0)
        if t + 1 == ROWS // 2:
            acc = acc + own_weight * own_value
        place = pl.ds(pl.multiple_of(slot + 16 * order[t], 16), 16)
        cx[place, :] = acc.astype(BF16)
        spread(3, lambda p: cx.at[place, :], cx.at[place, :])

    for copy in late_loads[:3]:
        copy.wait()
    second = jnp.zeros((8, 1), F32)
    for h in range(HEADS):
        second = jnp.where(sub[:, :1] == 2 * h, hsw[0:1, h : h + 1], second)
    gain = hg[...] * HEAD_SCALE
    square_mask = lax.rem(lax.broadcasted_iota(jnp.int32, (64, 128), 1), 64) == lax.broadcasted_iota(
        jnp.int32, (64, 128), 0
    )

    everything(2, sx.at[0 : KV - 1, :])
    stats = sx[...]
    factors = jnp.exp(stats - jnp.max(stats, axis=0, keepdims=True))
    weight_sum = jnp.sum(factors * pltpu.roll(stats, 64, 1), axis=0, keepdims=True)
    factors = factors * (1.0 / weight_sum)
    factors = jnp.where(low, factors[0:8], pltpu.roll(factors[8:16], DH, 1))
    high = factors.astype(BF16).astype(F32)
    mixing = jnp.concatenate(
        [
            jnp.concatenate(
                [jnp.where(square_mask, part[j : j + 1], 0.0).astype(BF16) for j in range(KV // 2)], axis=1
            )
            for part in (high, factors - high)
        ],
        axis=0,
    )
    everything(3, cx.at[0 : 64 * (KV - 1), :])
    both = jnp.dot(mixing, cx[...], preferred_element_type=F32)
    averaged = both[0:64] + both[64:128]
    for b in range(ROWS):
        one = averaged[8 * b : 8 * b + 8]
        difference = one - second * pltpu.roll(one, 7, 0)
        norm = lax.rsqrt(jnp.mean(difference * difference, axis=1, keepdims=True) + HEAD_EPSILON)
        df[8 * b : 8 * b + 8, :] = difference * norm * gain
    attended = jnp.concatenate([df[pl.ds(2 * h, 8, stride=8), :].astype(BF16) for h in range(HEADS)], axis=1)
    os_own[...] = jnp.dot(attended, ow_w[...], preferred_element_type=F32).astype(BF16)
    swap = pair(3, os_own, os_far)
    for copy in late_loads[3:]:
        copy.wait()
    swap.wait_recv()
    mixed = (tokens + (os_own[...].astype(F32) + os_far[...].astype(F32))).astype(BF16).astype(F32)
    mixer_scaled = (mixed * mixer_gain).astype(BF16)
    square = jnp.broadcast_to(jnp.sum(mixed * mixed, axis=1, keepdims=True), (8, 128))
    for w, ref in enumerate((gw_w, uw_w)):
        part = jnp.dot(mixer_scaled, ref[...], preferred_element_type=F32)
        for t in range(FT):
            row = (t // HT) * GR + w * HT + t % HT
            gs[pl.ds(row, 8, stride=2 * GR), :] = part[:, 128 * t : 128 * t + 128]
    high = square.astype(BF16).astype(F32)
    for half in range(2):
        gs[pl.ds(half * GR + 2 * HT, 8, stride=2 * GR), :] = high
        gs[pl.ds(half * GR + 2 * HT + 1, 8, stride=2 * GR), :] = square - high
    for j in range(KV):
        gb[j] = gs[j * GR : j * GR + GR, :].astype(BF16)
    gx[kv] = gb[kv]
    spread(5, lambda p: gb.at[p], gx.at[kv])
    everything(5, gx.at[0 : KV - 1])
    total = gx[0].astype(F32)
    for s in range(1, KV):
        total = total + gx[s].astype(F32)
    mixer_ratio = ratio_of(total[2 * HT : 2 * HT + 1] + total[2 * HT + 1 : 2 * HT + 2])
    gate = total[:HT] * mixer_ratio
    up = total[HT : 2 * HT] * mixer_ratio
    hidden = gate / (1.0 + jnp.exp(-gate)) * up
    mine = hx.at[KV * tp + kv, 0 : HT + 1]
    hx[KV * tp + kv, 0 : HT + 1, :] = jnp.concatenate([hidden, zero[0:1]], axis=0).astype(BF16)

    def share(p, core):
        pltpu.make_async_remote_copy(
            mine, mine, all_send.at[6], all_recv.at[6], device_id=(dp, p, core), device_id_type=MESH
        ).start()

    for p in peers:
        share(p, 1 - tp)
        share(p, tp)
    share(kv, 1 - tp)
    swap_down.wait_recv()
    everything(6, hx.at[0 : 2 * KV - 1, 0 : HT + 1])
    for s in range(2 * KV):
        hs[16 * s : 16 * s + 16, :] = hx[s].astype(F32)
    result = zero
    for core, weights in ((tp, dw_w), (1 - tp, dw_far)):
        at = pl.multiple_of(16 * KV * core, 8)
        hidden = jnp.concatenate(
            [
                jnp.concatenate([hs[pl.ds(at + 128 * k + t, 8, stride=16), :] for k in range(2)], axis=0).astype(BF16)
                for t in range(HT)
            ],
            axis=1,
        )
        down = jnp.concatenate([weights[0 : FF // 2, :], weights[FF // 2 : FF, :]], axis=1)
        part = jnp.dot(hidden, down, preferred_element_type=F32)
        ds[0:16, :] = part[:, 0:128]
        ds[16:32, :] = part[:, 128:256]
        part = ds[pl.ds(0, 8, stride=2), :] + ds[pl.ds(17, 8, stride=2), :]
        result = result + part.astype(BF16).astype(F32)
    result = mixed + result
    result = jnp.where(tp == 0, result, pltpu.roll(result, DH, 1))
    out_v[...] = result[:, :64].astype(BF16)
    store = pltpu.make_async_copy(out_v, out_ref, load_sem.at[len(loads)])
    store.start()
    for copy in sends + spreads:
        copy.wait_send()
    store.wait()


def shards(
    tokens, attention_gain, query_one, query_two, key_one, key_two, value_weight, head_second_weight, head_gain,
    out_weight, mixer_gain, gate_weight, up_weight, down_weight, key_cache, value_cache,
):
    any_space = pl.BlockSpec(memory_space=pl.ANY)
    vmem = pltpu.VMEM
    dma = pltpu.SemaphoreType.DMA
    return pl.pallas_call(
        layer_kernel,
        out_shape=jax.ShapeDtypeStruct((ROWS, 64), BF16),
        in_specs=[any_space] * 17,
        out_specs=any_space,
        scratch_shapes=[
            vmem((ROWS, 64), BF16), vmem((ROWS, 64), BF16),
            vmem((1, 64), BF16), vmem((1, 64), BF16), vmem((1, 64), BF16), vmem((1, 64), BF16),
            vmem((128, 256), BF16), vmem((128, 256), BF16), vmem((128, 256), BF16), vmem((128, 256), BF16),
            vmem((128, 512), BF16), vmem((1, HEADS), F32), vmem((1, 128), F32), vmem((512, 128), BF16),
            vmem((128, FF), BF16), vmem((128, FF), BF16), vmem((FF, 128), BF16),
            vmem((ROWS, KEYS, 128), BF16), vmem((ROWS, KEYS, 128), BF16), vmem((8, 128), F32),
            vmem((256, 256), BF16), vmem((ROWS // 2, 256, KEYS), BF16),
            vmem((KV, QR, 128), F32), vmem((KV * 8, 128), F32), vmem((KV, 8, 128), F32),
            vmem((KV * 64, 128), BF16), vmem((KV, 128), F32),
            vmem((KV * GR, 128), F32), vmem((KV, GR, 128), BF16), vmem((KV, GR, 128), BF16),
            vmem((2 * KV, 16, 128), BF16), vmem((2 * KV * 16, 128), F32), vmem((64, 128), F32),
            vmem((2, 16, KEYS), F32), vmem((64, 128), F32),
            vmem((8, 128), BF16), vmem((8, 128), BF16), vmem((FF, 128), BF16), vmem((32, 128), F32), vmem((ROWS, 64), BF16),
            pltpu.SemaphoreType.REGULAR((2,)), dma((18,)), dma((5,)), dma((5,)), dma((7,)), dma((7,)),
        ],
        compiler_params=pltpu.CompilerParams(
            collective_id=0, has_side_effects=True, vmem_limit_bytes=60 * 1024 * 1024
        ),
        name="layer",
    )(
        tokens, attention_gain.reshape(1, -1), query_one, query_two, key_one, key_two, value_weight,
        head_second_weight.reshape(1, -1), head_gain.reshape(1, -1), out_weight, mixer_gain.reshape(1, -1),
        gate_weight, up_weight, down_weight,
        key_cache.reshape(ROWS, KEYS, 128), value_cache.reshape(ROWS, KEYS, 128), jnp.asarray(rotary_tables()),
    )


def solution(mesh):
    both = ("kv", "tp")
    return jax.shard_map(
        shards,
        mesh=mesh,
        in_specs=(
            P("dp", both), P(both), P("kv", "tp"), P("kv", "tp"), P("kv", "tp"), P("kv", "tp"), P("kv", "tp"),
            P("tp"), P(), P("tp", "kv"), P(both), P("kv", "tp"), P("kv", "tp"), P("tp", "kv"),
            P("dp", "kv", "tp", None), P("dp", "kv", "tp", None),
        ),
        out_specs=P("dp", both),
        check_vma=False,
    )
```

```python
import jax
import jax.numpy as jnp
import numpy as np
from jax import lax
from jax.experimental import pallas as pl
from jax.experimental.pallas import tpu as pltpu
from jax.sharding import PartitionSpec as P

MESH = pl.DeviceIdType.MESH
F32 = jnp.float32
BF16 = jnp.bfloat16

D = 2048
DH = 64
POSITIONS = 1024
HEADS = 4
ROWS = 8
KV = 16
FF = 2816
FT = FF // 128
HT = FT // 2
CACHE = KV * POSITIONS
NORM_EPSILON = 1e-06
HEAD_EPSILON = 1e-05
HEAD_SCALE = 0.8
FLOOR = -1e30
LOG2E = 1.4426950408889634
KEYS = POSITIONS * HEADS
QR = 34
GR = 24


OFFSETS = sorted(
    ((i, j) for i in range(4) for j in range(4) if (i, j) != (0, 0)),
    key=lambda o: -min(o[0], 4 - o[0]) - min(o[1], 4 - o[1]),
)


def rotary_tables():
    half = DH // 2
    index = np.arange(half, dtype=np.float32) / np.float32(half)
    frequency = (np.float32(1.0) / np.power(np.float32(10000.0), index)).astype(np.float32)
    angle = (np.float32(CACHE) * frequency).astype(np.float32).astype(np.float64)
    cosine = np.tile(np.cos(angle).astype(np.float32), 4)
    sine = np.sin(angle).astype(np.float32)
    sine = np.tile(np.concatenate([-sine, sine]), 2)
    table = np.zeros((8, 128), np.float32)
    table[0], table[1] = cosine, sine
    return table


def layer_kernel(
    tok_h, ag_h, q1_h, q2_h, k1_h, k2_h, vw_h, hsw_h, hg_h, ow_h, mg_h, gw_h, uw_h, dw_h, kc_h, vc_h, tab_h,
    out_ref,
    tok_own, tok_far, ag_own, ag_far, mg_own, mg_far,
    q1_w, q2_w, k1_w, k2_w, vw_w, hsw, hg, ow_w, gw_w, uw_w, dw_w, kc, vc, tab,
    unit, kt, qx, rs, rx, cx, sx, gs, gb, gx, hx, hs, qs, sc, df, os_own, os_far, dw_far, ds, out_v,
    ready, load_sem, pair_send, pair_recv, all_send, all_recv,
):
    dp, kv, tp = (lax.axis_index(a) for a in ("dp", "kv", "tp"))
    barrier = pltpu.get_barrier_semaphore()
    partner = (dp, kv, 1 - tp)
    across, along = kv // 4, lax.rem(kv, 4)
    peers = [lax.rem(across + i, 4) * 4 + lax.rem(along + j, 4) for i, j in OFFSETS]
    for p in peers:
        pl.semaphore_signal(barrier, 1, device_id=(dp, p, 1), device_id_type=MESH)
    pl.semaphore_signal(barrier, 1, device_id=partner, device_id_type=MESH)

    loads = []

    def load(src, dst):
        copy = pltpu.make_async_copy(src, dst, load_sem.at[len(loads)])
        copy.start()
        loads.append(copy)
        return copy

    first = [load(a, b) for a, b in ((tok_h, tok_own), (ag_h, ag_own), (mg_h, mg_own))]
    q_loads = [load(a, b) for a, b in ((q1_h, q1_w), (q2_h, q2_w), (tab_h, tab))]
    down_load = load(dw_h, dw_w)
    kv_loads = [load(a, b) for a, b in ((k1_h, k1_w), (k2_h, k2_w), (vw_h, vw_w))]
    cache_loads = [load(kc_h, kc), load(vc_h, vc)]
    late_loads = [
        load(a, b)
        for a, b in ((hsw_h, hsw), (hg_h, hg), (ow_h, ow_w), (gw_h, gw_w), (uw_h, uw_w))
    ]
    @pl.when(tp == 0)
    def _():
        pl.semaphore_wait(barrier, 1)
        pl.semaphore_signal(ready.at[0], 1, device_id=partner, device_id_type=MESH)

    @pl.when(tp == 1)
    def _():
        pl.semaphore_wait(ready.at[0], 1)

    for copy in first:
        copy.wait()

    sends, spreads = [], []

    def pair(k, src, dst):
        copy = pltpu.make_async_remote_copy(
            src, dst, pair_send.at[k], pair_recv.at[k], device_id=partner, device_id_type=MESH
        )
        copy.start()
        sends.append(copy)
        return copy

    def spread(stage, source, target):
        for p in peers:
            pltpu.make_async_remote_copy(
                source(p), target, all_send.at[stage], all_recv.at[stage],
                device_id=(dp, p, tp), device_id_type=MESH,
            ).start()

    def everything(stage, most):
        copy = pltpu.make_async_remote_copy(
            most, most, all_send.at[stage], all_recv.at[stage], device_id=partner, device_id_type=MESH
        )
        spreads.append(copy)
        copy.wait_recv()

    swaps = [pair(0, tok_own, tok_far), pair(1, ag_own, ag_far), pair(2, mg_own, mg_far)]
    lane = lax.broadcasted_iota(jnp.int32, (8, 128), 1)
    sub = lax.broadcasted_iota(jnp.int32, (8, 128), 0)
    diagonal = lane == sub
    for copy in q_loads:
        copy.wait()
    down_load.wait()
    swap_down = pair(4, dw_w, dw_far)
    for copy in swaps:
        copy.wait_recv()

    def joined(own, far):
        own, far = own[...].astype(F32), far[...].astype(F32)
        return jnp.concatenate([jnp.where(tp == 0, own, far), jnp.where(tp == 0, far, own)], axis=-1)

    tokens = joined(tok_own, tok_far)
    scaled = (tokens * joined(ag_own, ag_far)).astype(BF16)
    mixer_gain = joined(mg_own, mg_far)
    square = jnp.sum(tokens * tokens, axis=1, keepdims=True)
    square_row = jnp.sum(jnp.where(diagonal, square, 0.0), axis=0, keepdims=True)
    for w, ref in enumerate((q1_w, q2_w)):
        part = jnp.dot(scaled, ref[...], preferred_element_type=F32)
        for t in range(2):
            qx[kv, 16 * w + 8 * t : 16 * w + 8 * t + 8, :] = part[:, 128 * t : 128 * t + 128].astype(BF16)
    high = square_row.astype(BF16).astype(F32)
    qx[kv, 32:34, :] = jnp.concatenate([high, square_row - high], axis=0).astype(BF16)
    for copy in kv_loads:
        copy.wait()
    for w, ref in enumerate((k1_w, k2_w)):
        part = jnp.dot(scaled, ref[...], preferred_element_type=F32)
        for t in range(2):
            rs[pl.ds(8 * t + w, 8, stride=16), :] = part[:, 128 * t : 128 * t + 128]
    part = jnp.dot(scaled, vw_w[...], preferred_element_type=F32)
    for t in range(HEADS):
        rs[pl.ds(8 * (t // 2) + 2 + t % 2, 8, stride=16), :] = part[:, 128 * t : 128 * t + 128]
    @pl.when(tp == 1)
    def _():
        pl.semaphore_wait(barrier, 2 * KV - 1)
        pl.semaphore_signal(ready.at[1], 1, device_id=partner, device_id_type=MESH)

    @pl.when(tp == 0)
    def _():
        pl.semaphore_wait(ready.at[1], 1)

    spread(0, lambda p: qx.at[kv], qx.at[kv])
    rx[kv] = rs[pl.ds(pl.multiple_of(8 * kv, 8), 8), :]
    spread(1, lambda p: rs.at[pl.ds(pl.multiple_of(8 * p, 8), 4), :], rx.at[kv, 0:4])

    wide = (256, 256)
    unit[...] = (lax.broadcasted_iota(jnp.int32, wide, 0) == lax.broadcasted_iota(jnp.int32, wide, 1)).astype(BF16)
    cache_loads[0].wait()

    def turn(c, carry):
        at = pl.multiple_of(c * 512, 512)
        for b in range(0, ROWS, 2):
            keys = jnp.concatenate([kc[b, pl.ds(at, 512), :], kc[b + 1, pl.ds(at, 512), :]], axis=1)
            turned = lax.dot_general(unit[...], keys, (((1,), (1,)), ((), ())), preferred_element_type=F32)
            kt[b // 2, :, pl.ds(at, 512)] = turned.astype(BF16)
        return carry

    lax.fori_loop(0, KEYS // 512, turn, 0)
    cache_loads[1].wait()
    everything(0, qx.at[0 : KV - 1])

    def ratio_of(total):
        return lax.rsqrt(total / D + NORM_EPSILON)

    square_total = qx[0, 32:34, :].astype(F32)
    for s in range(1, KV):
        square_total = square_total + qx[s, 32:34, :].astype(F32)
    square_total = jnp.sum(square_total, axis=0, keepdims=True)
    ratio_row = ratio_of(square_total)
    ratio = jnp.sum(jnp.where(diagonal, ratio_row, 0.0), axis=1, keepdims=True)
    cosine, sine = tab[0:1, :], tab[1:2, :]
    lead = lax.rem(lane, DH) < DH // 2

    def rotated(x):
        turned = jnp.where(lead, pltpu.roll(x, 128 - DH // 2, 1), pltpu.roll(x, DH // 2, 1))
        return (x * cosine + turned * sine).astype(BF16).astype(F32)

    def total_of(ref, at):
        total = ref[0, at : at + 8, :].astype(F32)
        for s in range(1, KV):
            total = total + ref[s, at : at + 8, :].astype(F32)
        return total

    query = [[rotated(total_of(qx, 16 * m + 8 * t) * ratio) for t in range(2)] for m in range(2)]
    low = lane < DH
    for h in range(HEADS):
        for m in range(2):
            x = query[m][h // 2]
            if h % 2 != m:
                x = pltpu.roll(x, DH, 1)
            qs[pl.ds(2 * h + m, 8, stride=8), :] = jnp.where(low if m == 0 else ~low, x, 0.0)

    key_head = lax.rem(lax.broadcasted_iota(jnp.int32, (16, 128), 1), HEADS)
    row_head = lax.rem(lax.broadcasted_iota(jnp.int32, (16, 128), 0), 8) // 2
    own_head = key_head == row_head
    scale = DH ** (-0.5)
    zero = jnp.zeros((8, 128), F32)
    step = 1024

    order = [lax.rem(across + 1 + t, 4) for t in range(ROWS // 2)]
    slot = 64 * (2 * lax.rem(kv, 8) + kv // 8)

    def score(t):
        rows = qs[pl.ds(pl.multiple_of(16 * order[t], 16), 16), :]
        left = jnp.concatenate(
            [
                jnp.concatenate([rows[0:8], zero], axis=1),
                jnp.concatenate([zero, rows[8:16]], axis=1),
            ],
            axis=0,
        ).astype(BF16)
        peak = jnp.full((16, 128), FLOOR, F32)
        for c in range(0, KEYS, step):
            s = jnp.dot(left, kt[order[t], :, c : c + step], preferred_element_type=F32)
            for i in range(0, step, 128):
                one = jnp.where(own_head, s[:, i : i + 128], FLOOR)
                peak = jnp.maximum(peak, one)
                sc[t % 2, :, c + i : c + i + 128] = one
        return jnp.max(peak, axis=1, keepdims=True)

    def new_token():
        everything(1, rx.at[0 : KV - 1, 0:4])
        row, share = kv // 2, lax.rem(kv, 2)
        new = total_of(rx, 0) * jnp.sum(jnp.where(sub[:, :1] == row, ratio, 0.0), axis=0, keepdims=True)
        asked = [
            jnp.sum(
                jnp.where(sub == row, jnp.where(share == 0, query[m][0], query[m][1]), 0.0), axis=0, keepdims=True
            )
            for m in range(2)
        ]
        product = jnp.where(sub == 0, asked[0], asked[1]) * rotated(new)
        wide_row = lax.broadcasted_iota(jnp.int32, (16, 128), 0)
        score_column = jnp.full((16, 1), FLOOR, F32)
        for k in range(2):
            half = jnp.sum(jnp.where(low if k == 0 else ~low, product, 0.0), axis=1, keepdims=True)
            for m in range(2):
                here = wide_row[:, :1] == 4 * along + 2 * k + m
                score_column = jnp.where(here, half[m : m + 1], score_column)
        new = new.astype(BF16).astype(F32)
        return score_column, jnp.where(lax.rem(wide_row, 4) < 2, new[2:3], new[3:4])

    stat = zero
    running = score(0)
    for t in range(ROWS // 2):
        b = 2 * order[t]
        peak = running
        if t + 1 < ROWS // 2:
            running = score(t + 1)
        else:
            own_score, own_value = new_token()
            peak = jnp.maximum(peak, own_score)
        total = jnp.zeros((16, 128), F32)
        weights = []
        for i in range(0, KEYS, 128):
            e = jnp.exp2((sc[t % 2, :, i : i + 128] - peak) * (scale * LOG2E))
            total = total + e
            weights.append(e.astype(BF16))
        total = jnp.sum(total, axis=1, keepdims=True)
        if t + 1 == ROWS // 2:
            own_weight = jnp.exp2((own_score - peak) * (scale * LOG2E))
            total = total + own_weight
        for k in range(2):
            at = 8 * (b + k)
            stat = jnp.where(lane - at == sub, peak[8 * k : 8 * k + 8] * scale, stat)
            stat = jnp.where(lane - 64 - at == sub, total[8 * k : 8 * k + 8], stat)
        if t + 1 == ROWS // 2:
            sx[pl.ds(kv, 1), :] = jnp.sum(stat, axis=0, keepdims=True)
            spread(2, lambda p: sx.at[pl.ds(kv, 1), :], sx.at[pl.ds(kv, 1), :])
        acc = jnp.zeros((16, 256), F32)
        for c in range(0, KEYS, step):
            values = jnp.concatenate([vc[b, c : c + step, :], vc[b + 1, c : c + step, :]], axis=1)
            w = jnp.concatenate(weights[c // 128 : (c + step) // 128], axis=1)
            acc = acc + jnp.dot(w, values, preferred_element_type=F32)
        acc = jnp.concatenate([acc[0:8, 0:128], acc[8:16, 128:256]], axis=0)
        if t + 1 == ROWS // 2:
            acc = acc + own_weight * own_value
        place = pl.ds(pl.multiple_of(slot + 16 * order[t], 16), 16)
        cx[place, :] = acc.astype(BF16)
        spread(3, lambda p: cx.at[place, :], cx.at[place, :])

    for copy in late_loads[:3]:
        copy.wait()
    second = jnp.zeros((8, 1), F32)
    for h in range(HEADS):
        second = jnp.where(sub[:, :1] == 2 * h, hsw[0:1, h : h + 1], second)
    gain = hg[...] * HEAD_SCALE
    square_mask = lax.rem(lax.broadcasted_iota(jnp.int32, (64, 128), 1), 64) == lax.broadcasted_iota(
        jnp.int32, (64, 128), 0
    )

    everything(2, sx.at[0 : KV - 1, :])
    stats = sx[...]
    factors = jnp.exp(stats - jnp.max(stats, axis=0, keepdims=True))
    weight_sum = jnp.sum(factors * pltpu.roll(stats, 64, 1), axis=0, keepdims=True)
    factors = factors * (1.0 / weight_sum)
    factors = jnp.where(low, factors[0:8], pltpu.roll(factors[8:16], DH, 1))
    high = factors.astype(BF16).astype(F32)
    mixing = jnp.concatenate(
        [
            jnp.concatenate(
                [jnp.where(square_mask, part[j : j + 1], 0.0).astype(BF16) for j in range(KV // 2)], axis=1
            )
            for part in (high, factors - high)
        ],
        axis=0,
    )
    everything(3, cx.at[0 : 64 * (KV - 1), :])
    both = jnp.dot(mixing, cx[...], preferred_element_type=F32)
    averaged = both[0:64] + both[64:128]
    for b in range(ROWS):
        one = averaged[8 * b : 8 * b + 8]
        difference = one - second * pltpu.roll(one, 7, 0)
        norm = lax.rsqrt(jnp.mean(difference * difference, axis=1, keepdims=True) + HEAD_EPSILON)
        df[8 * b : 8 * b + 8, :] = difference * norm * gain
    attended = jnp.concatenate([df[pl.ds(2 * h, 8, stride=8), :].astype(BF16) for h in range(HEADS)], axis=1)
    os_own[...] = jnp.dot(attended, ow_w[...], preferred_element_type=F32).astype(BF16)
    swap = pair(3, os_own, os_far)
    for copy in late_loads[3:]:
        copy.wait()
    swap.wait_recv()
    mixed = (tokens + (os_own[...].astype(F32) + os_far[...].astype(F32))).astype(BF16).astype(F32)
    mixer_scaled = (mixed * mixer_gain).astype(BF16)
    square = jnp.broadcast_to(jnp.sum(mixed * mixed, axis=1, keepdims=True), (8, 128))
    for w, ref in enumerate((gw_w, uw_w)):
        part = jnp.dot(mixer_scaled, ref[...], preferred_element_type=F32)
        for t in range(FT):
            row = (t // HT) * GR + w * HT + t % HT
            gs[pl.ds(row, 8, stride=2 * GR), :] = part[:, 128 * t : 128 * t + 128]
    high = square.astype(BF16).astype(F32)
    for half in range(2):
        gs[pl.ds(half * GR + 2 * HT, 8, stride=2 * GR), :] = high
        gs[pl.ds(half * GR + 2 * HT + 1, 8, stride=2 * GR), :] = square - high
    for j in range(KV):
        gb[j] = gs[j * GR : j * GR + GR, :].astype(BF16)
    gx[kv] = gb[kv]
    spread(5, lambda p: gb.at[p], gx.at[kv])
    everything(5, gx.at[0 : KV - 1])
    total = gx[0].astype(F32)
    for s in range(1, KV):
        total = total + gx[s].astype(F32)
    mixer_ratio = ratio_of(total[2 * HT : 2 * HT + 1] + total[2 * HT + 1 : 2 * HT + 2])
    gate = total[:HT] * mixer_ratio
    up = total[HT : 2 * HT] * mixer_ratio
    hidden = gate / (1.0 + jnp.exp(-gate)) * up
    mine = hx.at[KV * tp + kv, 0 : HT + 1]
    hx[KV * tp + kv, 0 : HT + 1, :] = jnp.concatenate([hidden, zero[0:1]], axis=0).astype(BF16)

    def share(p, core):
        pltpu.make_async_remote_copy(
            mine, mine, all_send.at[6], all_recv.at[6], device_id=(dp, p, core), device_id_type=MESH
        ).start()

    for p in peers:
        share(p, 1 - tp)
        share(p, tp)
    share(kv, 1 - tp)
    swap_down.wait_recv()
    everything(6, hx.at[0 : 2 * KV - 1, 0 : HT + 1])
    for s in range(2 * KV):
        hs[16 * s : 16 * s + 16, :] = hx[s].astype(F32)
    result = zero
    for core, weights in ((tp, dw_w), (1 - tp, dw_far)):
        at = pl.multiple_of(16 * KV * core, 8)
        hidden = jnp.concatenate(
            [
                jnp.concatenate([hs[pl.ds(at + 128 * k + t, 8, stride=16), :] for k in range(2)], axis=0).astype(BF16)
                for t in range(HT)
            ],
            axis=1,
        )
        down = jnp.concatenate([weights[0 : FF // 2, :], weights[FF // 2 : FF, :]], axis=1)
        part = jnp.dot(hidden, down, preferred_element_type=F32)
        ds[0:16, :] = part[:, 0:128]
        ds[16:32, :] = part[:, 128:256]
        part = ds[pl.ds(0, 8, stride=2), :] + ds[pl.ds(17, 8, stride=2), :]
        result = result + part.astype(BF16).astype(F32)
    result = mixed + result
    result = jnp.where(tp == 0, result, pltpu.roll(result, DH, 1))
    out_ref[...] = result[:, :64].astype(BF16)
    for copy in sends + spreads:
        copy.wait_send()


def shards(
    tokens, attention_gain, query_one, query_two, key_one, key_two, value_weight, head_second_weight, head_gain,
    out_weight, mixer_gain, gate_weight, up_weight, down_weight, key_cache, value_cache,
):
    any_space = pl.BlockSpec(memory_space=pl.ANY)
    vmem = pltpu.VMEM
    dma = pltpu.SemaphoreType.DMA
    return pl.pallas_call(
        layer_kernel,
        out_shape=pltpu.VMEM((ROWS, 64), BF16),
        in_specs=[any_space] * 17,
        out_specs=pl.BlockSpec(memory_space=pltpu.VMEM),
        scratch_shapes=[
            vmem((ROWS, 64), BF16), vmem((ROWS, 64), BF16),
            vmem((1, 64), BF16), vmem((1, 64), BF16), vmem((1, 64), BF16), vmem((1, 64), BF16),
            vmem((128, 256), BF16), vmem((128, 256), BF16), vmem((128, 256), BF16), vmem((128, 256), BF16),
            vmem((128, 512), BF16), vmem((1, HEADS), F32), vmem((1, 128), F32), vmem((512, 128), BF16),
            vmem((128, FF), BF16), vmem((128, FF), BF16), vmem((FF, 128), BF16),
            vmem((ROWS, KEYS, 128), BF16), vmem((ROWS, KEYS, 128), BF16), vmem((8, 128), F32),
            vmem((256, 256), BF16), vmem((ROWS // 2, 256, KEYS), BF16),
            vmem((KV, QR, 128), BF16), vmem((KV * 8, 128), F32), vmem((KV, 8, 128), F32),
            vmem((KV * 64, 128), BF16), vmem((KV, 128), F32),
            vmem((KV * GR, 128), F32), vmem((KV, GR, 128), BF16), vmem((KV, GR, 128), BF16),
            vmem((2 * KV, 16, 128), BF16), vmem((2 * KV * 16, 128), F32), vmem((64, 128), F32),
            vmem((2, 16, KEYS), F32), vmem((64, 128), F32),
            vmem((8, 128), BF16), vmem((8, 128), BF16), vmem((FF, 128), BF16), vmem((32, 128), F32), vmem((ROWS, 64), BF16),
            pltpu.SemaphoreType.REGULAR((2,)), dma((18,)), dma((5,)), dma((5,)), dma((7,)), dma((7,)),
        ],
        compiler_params=pltpu.CompilerParams(
            collective_id=0, has_side_effects=True, vmem_limit_bytes=60 * 1024 * 1024
        ),
        name="layer",
    )(
        tokens, attention_gain.reshape(1, -1), query_one, query_two, key_one, key_two, value_weight,
        head_second_weight.reshape(1, -1), head_gain.reshape(1, -1), out_weight, mixer_gain.reshape(1, -1),
        gate_weight, up_weight, down_weight,
        key_cache.reshape(ROWS, KEYS, 128), value_cache.reshape(ROWS, KEYS, 128), jnp.asarray(rotary_tables()),
    )


def solution(mesh):
    both = ("kv", "tp")
    return jax.shard_map(
        shards,
        mesh=mesh,
        in_specs=(
            P("dp", both), P(both), P("kv", "tp"), P("kv", "tp"), P("kv", "tp"), P("kv", "tp"), P("kv", "tp"),
            P("tp"), P(), P("tp", "kv"), P(both), P("kv", "tp"), P("kv", "tp"), P("tp", "kv"),
            P("dp", "kv", "tp", None), P("dp", "kv", "tp", None),
        ),
        out_specs=P("dp", both),
        check_vma=False,
    )
```

```python
import jax
import jax.numpy as jnp
import numpy as np
from jax import lax
from jax.experimental import pallas as pl
from jax.experimental.pallas import tpu as pltpu
from jax.sharding import PartitionSpec as P

MESH = pl.DeviceIdType.MESH
F32 = jnp.float32
BF16 = jnp.bfloat16

D = 2048
DH = 64
POSITIONS = 1024
HEADS = 4
ROWS = 8
KV = 16
FF = 2816
FT = FF // 128
HT = FT // 2
CACHE = KV * POSITIONS
NORM_EPSILON = 1e-06
HEAD_EPSILON = 1e-05
HEAD_SCALE = 0.8
FLOOR = -1e30
LOG2E = 1.4426950408889634
KEYS = POSITIONS * HEADS
QR = 33
GR = 24


OFFSETS = (
    (2, 2), (3, 2), (2, 3), (1, 2), (2, 1), (3, 3), (3, 1), (1, 3), (1, 1), (0, 2), (2, 0), (0, 3), (3, 0), (0, 1), (1, 0),
)


def rotary_tables():
    half = DH // 2
    index = np.arange(half, dtype=np.float32) / np.float32(half)
    frequency = (np.float32(1.0) / np.power(np.float32(10000.0), index)).astype(np.float32)
    angle = (np.float32(CACHE) * frequency).astype(np.float32).astype(np.float64)
    cosine = np.tile(np.cos(angle).astype(np.float32), 4)
    sine = np.sin(angle).astype(np.float32)
    sine = np.tile(np.concatenate([-sine, sine]), 2)
    table = np.zeros((8, 128), np.float32)
    table[0], table[1] = cosine, sine
    return table


def layer_kernel(
    tok_h, ag_h, q1_h, q2_h, k1_h, k2_h, vw_h, hsw_h, hg_h, ow_h, mg_h, gw_h, uw_h, dw_h, kc_h, vc_h, tab_h,
    out_ref,
    tok_own, tok_far, ag_own, ag_far, mg_own, mg_far,
    q1_w, q2_w, k1_w, k2_w, vw_w, hsw, hg, ow_w, gw_w, uw_w, dw_w, kc, vc, tab,
    unit, kt, qx, rs, rx, cx, sx, gs, gb, gx, hx, hs, qs, sc, df, os_own, os_far, dw_far, ds,
    ready, load_sem, pair_send, pair_recv, all_send, all_recv,
):
    dp, kv, tp = (lax.axis_index(a) for a in ("dp", "kv", "tp"))
    barrier = pltpu.get_barrier_semaphore()
    partner = (dp, kv, 1 - tp)
    across, along = kv // 4, lax.rem(kv, 4)
    peers = [lax.rem(across + i, 4) * 4 + lax.rem(along + j, 4) for i, j in OFFSETS]
    for p in peers:
        pl.semaphore_signal(barrier, 1, device_id=(dp, p, 1), device_id_type=MESH)
    pl.semaphore_signal(barrier, 1, device_id=partner, device_id_type=MESH)

    loads = []

    def load(src, dst):
        copy = pltpu.make_async_copy(src, dst, load_sem.at[len(loads)])
        copy.start()
        loads.append(copy)
        return copy

    first = [load(a, b) for a, b in ((tok_h, tok_own), (ag_h, ag_own), (mg_h, mg_own))]
    q_loads = [load(a, b) for a, b in ((q1_h, q1_w), (q2_h, q2_w), (tab_h, tab))]
    down_load = load(dw_h, dw_w)
    kv_loads = [load(a, b) for a, b in ((k1_h, k1_w), (k2_h, k2_w), (vw_h, vw_w))]
    cache_loads = [load(kc_h, kc), load(vc_h, vc)]
    late_loads = [
        load(a, b)
        for a, b in ((hsw_h, hsw), (hg_h, hg), (ow_h, ow_w), (gw_h, gw_w), (uw_h, uw_w))
    ]
    @pl.when(tp == 0)
    def _():
        pl.semaphore_wait(barrier, 1)
        pl.semaphore_signal(ready.at[0], 1, device_id=partner, device_id_type=MESH)

    @pl.when(tp == 1)
    def _():
        pl.semaphore_wait(ready.at[0], 1)

    for copy in first:
        copy.wait()

    sends, spreads = [], []

    def pair(k, src, dst):
        copy = pltpu.make_async_remote_copy(
            src, dst, pair_send.at[k], pair_recv.at[k], device_id=partner, device_id_type=MESH
        )
        copy.start()
        sends.append(copy)
        return copy

    def spread(stage, source, target):
        for p in peers:
            pltpu.make_async_remote_copy(
                source(p), target, all_send.at[stage], all_recv.at[stage],
                device_id=(dp, p, tp), device_id_type=MESH,
            ).start()

    def everything(stage, most):
        copy = pltpu.make_async_remote_copy(
            most, most, all_send.at[stage], all_recv.at[stage], device_id=partner, device_id_type=MESH
        )
        spreads.append(copy)
        copy.wait_recv()

    swaps = [pair(0, tok_own, tok_far), pair(1, ag_own, ag_far), pair(2, mg_own, mg_far)]
    lane = lax.broadcasted_iota(jnp.int32, (8, 128), 1)
    sub = lax.broadcasted_iota(jnp.int32, (8, 128), 0)
    diagonal = lane == sub
    for copy in q_loads:
        copy.wait()
    down_load.wait()
    swap_down = pair(4, dw_w, dw_far)
    for copy in swaps:
        copy.wait_recv()

    def joined(own, far):
        own, far = own[...].astype(F32), far[...].astype(F32)
        return jnp.concatenate([jnp.where(tp == 0, own, far), jnp.where(tp == 0, far, own)], axis=-1)

    tokens = joined(tok_own, tok_far)
    scaled = (tokens * joined(ag_own, ag_far)).astype(BF16)
    mixer_gain = joined(mg_own, mg_far)
    square = jnp.sum(tokens * tokens, axis=1, keepdims=True)
    square_row = jnp.sum(jnp.where(diagonal, square, 0.0), axis=0, keepdims=True)
    for w, ref in enumerate((q1_w, q2_w)):
        part = jnp.dot(scaled, ref[...], preferred_element_type=F32)
        for t in range(2):
            qx[kv, 16 * w + 8 * t : 16 * w + 8 * t + 8, :] = part[:, 128 * t : 128 * t + 128]
    qx[kv, 32:33, :] = square_row
    for copy in kv_loads:
        copy.wait()
    for w, ref in enumerate((k1_w, k2_w)):
        part = jnp.dot(scaled, ref[...], preferred_element_type=F32)
        for t in range(2):
            rs[pl.ds(8 * t + w, 8, stride=16), :] = part[:, 128 * t : 128 * t + 128]
    part = jnp.dot(scaled, vw_w[...], preferred_element_type=F32)
    for t in range(HEADS):
        rs[pl.ds(8 * (t // 2) + 2 + t % 2, 8, stride=16), :] = part[:, 128 * t : 128 * t + 128]
    @pl.when(tp == 1)
    def _():
        pl.semaphore_wait(barrier, 2 * KV - 1)
        pl.semaphore_signal(ready.at[1], 1, device_id=partner, device_id_type=MESH)

    @pl.when(tp == 0)
    def _():
        pl.semaphore_wait(ready.at[1], 1)

    spread(0, lambda p: qx.at[kv], qx.at[kv])
    rx[kv] = rs[pl.ds(pl.multiple_of(8 * kv, 8), 8), :]
    spread(1, lambda p: rs.at[pl.ds(pl.multiple_of(8 * p, 8), 4), :], rx.at[kv, 0:4])

    wide = (256, 256)
    unit[...] = (lax.broadcasted_iota(jnp.int32, wide, 0) == lax.broadcasted_iota(jnp.int32, wide, 1)).astype(BF16)
    cache_loads[0].wait()

    def turn(c, carry):
        at = pl.multiple_of(c * 512, 512)
        for b in range(0, ROWS, 2):
            keys = jnp.concatenate([kc[b, pl.ds(at, 512), :], kc[b + 1, pl.ds(at, 512), :]], axis=1)
            turned = lax.dot_general(unit[...], keys, (((1,), (1,)), ((), ())), preferred_element_type=F32)
            kt[b // 2, :, pl.ds(at, 512)] = turned.astype(BF16)
        return carry

    lax.fori_loop(0, KEYS // 512, turn, 0)
    cache_loads[1].wait()
    everything(0, qx.at[0 : KV - 1])

    def ratio_of(total):
        return lax.rsqrt(total / D + NORM_EPSILON)

    square_total = qx[0, 32:33, :]
    for s in range(1, KV):
        square_total = square_total + qx[s, 32:33, :]
    ratio_row = ratio_of(square_total)
    ratio = jnp.sum(jnp.where(diagonal, ratio_row, 0.0), axis=1, keepdims=True)
    cosine, sine = tab[0:1, :], tab[1:2, :]
    lead = lax.rem(lane, DH) < DH // 2

    def rotated(x):
        turned = jnp.where(lead, pltpu.roll(x, 128 - DH // 2, 1), pltpu.roll(x, DH // 2, 1))
        return (x * cosine + turned * sine).astype(BF16).astype(F32)

    def total_of(ref, at):
        total = ref[0, at : at + 8, :]
        for s in range(1, KV):
            total = total + ref[s, at : at + 8, :]
        return total

    query = [[rotated(total_of(qx, 16 * m + 8 * t) * ratio) for t in range(2)] for m in range(2)]
    low = lane < DH
    for h in range(HEADS):
        for m in range(2):
            x = query[m][h // 2]
            if h % 2 != m:
                x = pltpu.roll(x, DH, 1)
            qs[pl.ds(2 * h + m, 8, stride=8), :] = jnp.where(low if m == 0 else ~low, x, 0.0)

    key_head = lax.rem(lax.broadcasted_iota(jnp.int32, (16, 128), 1), HEADS)
    row_head = lax.rem(lax.broadcasted_iota(jnp.int32, (16, 128), 0), 8) // 2
    own_head = key_head == row_head
    scale = DH ** (-0.5)
    zero = jnp.zeros((8, 128), F32)
    step = 1024

    order = [lax.rem(across + 1 + t, 4) for t in range(ROWS // 2)]
    slot = 64 * (2 * lax.rem(kv, 8) + kv // 8)

    def score(t):
        rows = qs[pl.ds(pl.multiple_of(16 * order[t], 16), 16), :]
        left = jnp.concatenate(
            [
                jnp.concatenate([rows[0:8], zero], axis=1),
                jnp.concatenate([zero, rows[8:16]], axis=1),
            ],
            axis=0,
        ).astype(BF16)
        peak = jnp.full((16, 128), FLOOR, F32)
        for c in range(0, KEYS, step):
            s = jnp.dot(left, kt[order[t], :, c : c + step], preferred_element_type=F32)
            for i in range(0, step, 128):
                one = jnp.where(own_head, s[:, i : i + 128], FLOOR)
                peak = jnp.maximum(peak, one)
                sc[t % 2, :, c + i : c + i + 128] = one
        return jnp.max(peak, axis=1, keepdims=True)

    def new_token():
        everything(1, rx.at[0 : KV - 1, 0:4])
        row, share = kv // 2, lax.rem(kv, 2)
        new = total_of(rx, 0) * jnp.sum(jnp.where(sub[:, :1] == row, ratio, 0.0), axis=0, keepdims=True)
        asked = [
            jnp.sum(
                jnp.where(sub == row, jnp.where(share == 0, query[m][0], query[m][1]), 0.0), axis=0, keepdims=True
            )
            for m in range(2)
        ]
        product = jnp.where(sub == 0, asked[0], asked[1]) * rotated(new)
        wide_row = lax.broadcasted_iota(jnp.int32, (16, 128), 0)
        score_column = jnp.full((16, 1), FLOOR, F32)
        for k in range(2):
            half = jnp.sum(jnp.where(low if k == 0 else ~low, product, 0.0), axis=1, keepdims=True)
            for m in range(2):
                here = wide_row[:, :1] == 4 * along + 2 * k + m
                score_column = jnp.where(here, half[m : m + 1], score_column)
        new = new.astype(BF16).astype(F32)
        return score_column, jnp.where(lax.rem(wide_row, 4) < 2, new[2:3], new[3:4])

    stat = zero
    running = score(0)
    for t in range(ROWS // 2):
        b = 2 * order[t]
        peak = running
        if t + 1 < ROWS // 2:
            running = score(t + 1)
        else:
            own_score, own_value = new_token()
            peak = jnp.maximum(peak, own_score)
        total = jnp.zeros((16, 128), F32)
        weights = []
        for i in range(0, KEYS, 128):
            e = jnp.exp2((sc[t % 2, :, i : i + 128] - peak) * (scale * LOG2E))
            total = total + e
            weights.append(e.astype(BF16))
        total = jnp.sum(total, axis=1, keepdims=True)
        if t + 1 == ROWS // 2:
            own_weight = jnp.exp2((own_score - peak) * (scale * LOG2E))
            total = total + own_weight
        for k in range(2):
            at = 8 * (b + k)
            stat = jnp.where(lane - at == sub, peak[8 * k : 8 * k + 8] * scale, stat)
            stat = jnp.where(lane - 64 - at == sub, total[8 * k : 8 * k + 8], stat)
        if t + 1 == ROWS // 2:
            sx[pl.ds(kv, 1), :] = jnp.sum(stat, axis=0, keepdims=True)
            spread(2, lambda p: sx.at[pl.ds(kv, 1), :], sx.at[pl.ds(kv, 1), :])
        acc = jnp.zeros((16, 256), F32)
        for c in range(0, KEYS, step):
            values = jnp.concatenate([vc[b, c : c + step, :], vc[b + 1, c : c + step, :]], axis=1)
            w = jnp.concatenate(weights[c // 128 : (c + step) // 128], axis=1)
            acc = acc + jnp.dot(w, values, preferred_element_type=F32)
        acc = jnp.concatenate([acc[0:8, 0:128], acc[8:16, 128:256]], axis=0)
        if t + 1 == ROWS // 2:
            acc = acc + own_weight * own_value
        place = pl.ds(pl.multiple_of(slot + 16 * order[t], 16), 16)
        cx[place, :] = acc.astype(BF16)
        spread(3, lambda p: cx.at[place, :], cx.at[place, :])

    for copy in late_loads[:3]:
        copy.wait()
    second = jnp.zeros((8, 1), F32)
    for h in range(HEADS):
        second = jnp.where(sub[:, :1] == 2 * h, hsw[0:1, h : h + 1], second)
    gain = hg[...] * HEAD_SCALE
    square_mask = lax.rem(lax.broadcasted_iota(jnp.int32, (64, 128), 1), 64) == lax.broadcasted_iota(
        jnp.int32, (64, 128), 0
    )

    everything(2, sx.at[0 : KV - 1, :])
    stats = sx[...]
    factors = jnp.exp(stats - jnp.max(stats, axis=0, keepdims=True))
    weight_sum = jnp.sum(factors * pltpu.roll(stats, 64, 1), axis=0, keepdims=True)
    factors = factors * (1.0 / weight_sum)
    factors = jnp.where(low, factors[0:8], pltpu.roll(factors[8:16], DH, 1))
    high = factors.astype(BF16).astype(F32)
    mixing = jnp.concatenate(
        [
            jnp.concatenate(
                [jnp.where(square_mask, part[j : j + 1], 0.0).astype(BF16) for j in range(KV // 2)], axis=1
            )
            for part in (high, factors - high)
        ],
        axis=0,
    )
    everything(3, cx.at[0 : 64 * (KV - 1), :])
    both = jnp.dot(mixing, cx[...], preferred_element_type=F32)
    averaged = both[0:64] + both[64:128]
    for b in range(ROWS):
        one = averaged[8 * b : 8 * b + 8]
        difference = one - second * pltpu.roll(one, 7, 0)
        norm = lax.rsqrt(jnp.mean(difference * difference, axis=1, keepdims=True) + HEAD_EPSILON)
        df[8 * b : 8 * b + 8, :] = difference * norm * gain
    attended = jnp.concatenate([df[pl.ds(2 * h, 8, stride=8), :].astype(BF16) for h in range(HEADS)], axis=1)
    os_own[...] = jnp.dot(attended, ow_w[...], preferred_element_type=F32).astype(BF16)
    swap = pair(3, os_own, os_far)
    for copy in late_loads[3:]:
        copy.wait()
    swap.wait_recv()
    mixed = (tokens + (os_own[...].astype(F32) + os_far[...].astype(F32))).astype(BF16).astype(F32)
    mixer_scaled = (mixed * mixer_gain).astype(BF16)
    square = jnp.broadcast_to(jnp.sum(mixed * mixed, axis=1, keepdims=True), (8, 128))
    for w, ref in enumerate((gw_w, uw_w)):
        part = jnp.dot(mixer_scaled, ref[...], preferred_element_type=F32)
        for t in range(FT):
            row = (t // HT) * GR + w * HT + t % HT
            gs[pl.ds(row, 8, stride=2 * GR), :] = part[:, 128 * t : 128 * t + 128]
    high = square.astype(BF16).astype(F32)
    for half in range(2):
        gs[pl.ds(half * GR + 2 * HT, 8, stride=2 * GR), :] = high
        gs[pl.ds(half * GR + 2 * HT + 1, 8, stride=2 * GR), :] = square - high
    for j in range(KV):
        gb[j] = gs[j * GR : j * GR + GR, :].astype(BF16)
    gx[kv] = gb[kv]
    spread(5, lambda p: gb.at[p], gx.at[kv])
    everything(5, gx.at[0 : KV - 1])
    total = gx[0].astype(F32)
    for s in range(1, KV):
        total = total + gx[s].astype(F32)
    mixer_ratio = ratio_of(total[2 * HT : 2 * HT + 1] + total[2 * HT + 1 : 2 * HT + 2])
    gate = total[:HT] * mixer_ratio
    up = total[HT : 2 * HT] * mixer_ratio
    hidden = gate / (1.0 + jnp.exp(-gate)) * up
    mine = hx.at[KV * tp + kv, 0 : HT + 1]
    hx[KV * tp + kv, 0 : HT + 1, :] = jnp.concatenate([hidden, zero[0:1]], axis=0).astype(BF16)

    def share(p, core):
        pltpu.make_async_remote_copy(
            mine, mine, all_send.at[6], all_recv.at[6], device_id=(dp, p, core), device_id_type=MESH
        ).start()

    for p in peers:
        share(p, 1 - tp)
        share(p, tp)
    share(kv, 1 - tp)
    swap_down.wait_recv()
    everything(6, hx.at[0 : 2 * KV - 1, 0 : HT + 1])
    for s in range(2 * KV):
        hs[16 * s : 16 * s + 16, :] = hx[s].astype(F32)
    result = zero
    for core, weights in ((tp, dw_w), (1 - tp, dw_far)):
        at = pl.multiple_of(16 * KV * core, 8)
        hidden = jnp.concatenate(
            [
                jnp.concatenate([hs[pl.ds(at + 128 * k + t, 8, stride=16), :] for k in range(2)], axis=0).astype(BF16)
                for t in range(HT)
            ],
            axis=1,
        )
        down = jnp.concatenate([weights[0 : FF // 2, :], weights[FF // 2 : FF, :]], axis=1)
        part = jnp.dot(hidden, down, preferred_element_type=F32)
        ds[0:16, :] = part[:, 0:128]
        ds[16:32, :] = part[:, 128:256]
        part = ds[pl.ds(0, 8, stride=2), :] + ds[pl.ds(17, 8, stride=2), :]
        result = result + part.astype(BF16).astype(F32)
    result = mixed + result
    result = jnp.where(tp == 0, result, pltpu.roll(result, DH, 1))
    out_ref[...] = result[:, :64].astype(BF16)
    for copy in sends + spreads:
        copy.wait_send()


def shards(
    tokens, attention_gain, query_one, query_two, key_one, key_two, value_weight, head_second_weight, head_gain,
    out_weight, mixer_gain, gate_weight, up_weight, down_weight, key_cache, value_cache,
):
    any_space = pl.BlockSpec(memory_space=pl.ANY)
    vmem = pltpu.VMEM
    dma = pltpu.SemaphoreType.DMA
    return pl.pallas_call(
        layer_kernel,
        out_shape=pltpu.VMEM((ROWS, 64), BF16),
        in_specs=[any_space] * 17,
        out_specs=pl.BlockSpec(memory_space=pltpu.VMEM),
        scratch_shapes=[
            vmem((ROWS, 64), BF16), vmem((ROWS, 64), BF16),
            vmem((1, 64), BF16), vmem((1, 64), BF16), vmem((1, 64), BF16), vmem((1, 64), BF16),
            vmem((128, 256), BF16), vmem((128, 256), BF16), vmem((128, 256), BF16), vmem((128, 256), BF16),
            vmem((128, 512), BF16), vmem((1, HEADS), F32), vmem((1, 128), F32), vmem((512, 128), BF16),
            vmem((128, FF), BF16), vmem((128, FF), BF16), vmem((FF, 128), BF16),
            vmem((ROWS, KEYS, 128), BF16), vmem((ROWS, KEYS, 128), BF16), vmem((8, 128), F32),
            vmem((256, 256), BF16), vmem((ROWS // 2, 256, KEYS), BF16),
            vmem((KV, QR, 128), F32), vmem((KV * 8, 128), F32), vmem((KV, 8, 128), F32),
            vmem((KV * 64, 128), BF16), vmem((KV, 128), F32),
            vmem((KV * GR, 128), F32), vmem((KV, GR, 128), BF16), vmem((KV, GR, 128), BF16),
            vmem((2 * KV, 16, 128), BF16), vmem((2 * KV * 16, 128), F32), vmem((64, 128), F32),
            vmem((2, 16, KEYS), F32), vmem((64, 128), F32),
            vmem((8, 128), BF16), vmem((8, 128), BF16), vmem((FF, 128), BF16), vmem((32, 128), F32),
            pltpu.SemaphoreType.REGULAR((2,)), dma((17,)), dma((5,)), dma((5,)), dma((7,)), dma((7,)),
        ],
        compiler_params=pltpu.CompilerParams(
            collective_id=0, has_side_effects=True, vmem_limit_bytes=60 * 1024 * 1024
        ),
        name="layer",
    )(
        tokens, attention_gain.reshape(1, -1), query_one, query_two, key_one, key_two, value_weight,
        head_second_weight.reshape(1, -1), head_gain.reshape(1, -1), out_weight, mixer_gain.reshape(1, -1),
        gate_weight, up_weight, down_weight,
        key_cache.reshape(ROWS, KEYS, 128), value_cache.reshape(ROWS, KEYS, 128), jnp.asarray(rotary_tables()),
    )


def solution(mesh):
    both = ("kv", "tp")
    return jax.shard_map(
        shards,
        mesh=mesh,
        in_specs=(
            P("dp", both), P(both), P("kv", "tp"), P("kv", "tp"), P("kv", "tp"), P("kv", "tp"), P("kv", "tp"),
            P("tp"), P(), P("tp", "kv"), P(both), P("kv", "tp"), P("kv", "tp"), P("tp", "kv"),
            P("dp", "kv", "tp", None), P("dp", "kv", "tp", None),
        ),
        out_specs=P("dp", both),
        check_vma=False,
    )
```

```python
import jax
import jax.numpy as jnp
import numpy as np
from jax import lax
from jax.experimental import pallas as pl
from jax.experimental.pallas import tpu as pltpu
from jax.sharding import PartitionSpec as P

MESH = pl.DeviceIdType.MESH
F32 = jnp.float32
BF16 = jnp.bfloat16

D = 2048
DH = 64
POSITIONS = 1024
HEADS = 4
ROWS = 8
KV = 16
FF = 2816
FT = FF // 128
HT = FT // 2
CACHE = KV * POSITIONS
NORM_EPSILON = 1e-06
HEAD_EPSILON = 1e-05
HEAD_SCALE = 0.8
FLOOR = -1e30
LOG2E = 1.4426950408889634
KEYS = POSITIONS * HEADS
QR = 33
GR = 24


OFFSETS = (
    (2, 2), (3, 2), (2, 3), (1, 2), (2, 1), (3, 3), (3, 1), (1, 3), (1, 1), (0, 2), (2, 0), (0, 3), (3, 0), (0, 1), (1, 0),
)


def rotary_tables():
    half = DH // 2
    index = np.arange(half, dtype=np.float32) / np.float32(half)
    frequency = (np.float32(1.0) / np.power(np.float32(10000.0), index)).astype(np.float32)
    angle = (np.float32(CACHE) * frequency).astype(np.float32).astype(np.float64)
    cosine = np.tile(np.cos(angle).astype(np.float32), 4)
    sine = np.sin(angle).astype(np.float32)
    sine = np.tile(np.concatenate([-sine, sine]), 2)
    table = np.zeros((8, 128), np.float32)
    table[0], table[1] = cosine, sine
    return table


def layer_kernel(
    tok_h, ag_h, q1_h, q2_h, k1_h, k2_h, vw_h, hsw_h, hg_h, ow_h, mg_h, gw_h, uw_h, dw_h, kc_h, vc_h, tab_h,
    out_ref,
    tok_own, tok_far, ag_own, ag_far, mg_own, mg_far,
    q1_w, q2_w, k1_w, k2_w, vw_w, hsw, hg, ow_w, gw_w, uw_w, dw_w, kc, vc, tab,
    unit, kt, qx, rs, rx, cx, sx, gs, gb, gx, hx, hs, qs, sc, df, os_own, os_far, dw_far, ds,
    ready, load_sem, pair_send, pair_recv, all_send, all_recv,
):
    dp, kv, tp = (lax.axis_index(a) for a in ("dp", "kv", "tp"))
    barrier = pltpu.get_barrier_semaphore()
    partner = (dp, kv, 1 - tp)
    across, along = kv // 4, lax.rem(kv, 4)
    peers = [lax.rem(across + i, 4) * 4 + lax.rem(along + j, 4) for i, j in OFFSETS]
    for p in peers:
        pl.semaphore_signal(barrier, 1, device_id=(dp, p, 1), device_id_type=MESH)
    pl.semaphore_signal(barrier, 1, device_id=partner, device_id_type=MESH)

    loads = []

    def load(src, dst):
        copy = pltpu.make_async_copy(src, dst, load_sem.at[len(loads)])
        copy.start()
        loads.append(copy)
        return copy

    first = [load(a, b) for a, b in ((tok_h, tok_own), (ag_h, ag_own), (mg_h, mg_own))]
    q_loads = [load(a, b) for a, b in ((q1_h, q1_w), (q2_h, q2_w), (tab_h, tab))]
    down_load = load(dw_h, dw_w)
    kv_loads = [load(a, b) for a, b in ((k1_h, k1_w), (k2_h, k2_w), (vw_h, vw_w))]
    cache_loads = [load(kc_h, kc), load(vc_h, vc)]
    late_loads = [
        load(a, b)
        for a, b in ((hsw_h, hsw), (hg_h, hg), (ow_h, ow_w), (gw_h, gw_w), (uw_h, uw_w))
    ]
    @pl.when(tp == 0)
    def _():
        pl.semaphore_wait(barrier, 1)
        pl.semaphore_signal(ready.at[0], 1, device_id=partner, device_id_type=MESH)

    @pl.when(tp == 1)
    def _():
        pl.semaphore_wait(ready.at[0], 1)

    for copy in first:
        copy.wait()

    sends, spreads = [], []

    def pair(k, src, dst):
        copy = pltpu.make_async_remote_copy(
            src, dst, pair_send.at[k], pair_recv.at[k], device_id=partner, device_id_type=MESH
        )
        copy.start()
        sends.append(copy)
        return copy

    def spread(stage, source, target):
        for p in peers:
            pltpu.make_async_remote_copy(
                source(p), target, all_send.at[stage], all_recv.at[stage],
                device_id=(dp, p, tp), device_id_type=MESH,
            ).start()

    def everything(stage, most):
        copy = pltpu.make_async_remote_copy(
            most, most, all_send.at[stage], all_recv.at[stage], device_id=partner, device_id_type=MESH
        )
        spreads.append(copy)
        copy.wait_recv()

    swaps = [pair(0, tok_own, tok_far), pair(1, ag_own, ag_far), pair(2, mg_own, mg_far)]
    lane = lax.broadcasted_iota(jnp.int32, (8, 128), 1)
    sub = lax.broadcasted_iota(jnp.int32, (8, 128), 0)
    diagonal = lane == sub
    for copy in q_loads:
        copy.wait()
    down_load.wait()
    swap_down = pair(4, dw_w, dw_far)
    for copy in swaps:
        copy.wait_recv()

    def joined(own, far):
        own, far = own[...].astype(F32), far[...].astype(F32)
        return jnp.concatenate([jnp.where(tp == 0, own, far), jnp.where(tp == 0, far, own)], axis=-1)

    tokens = joined(tok_own, tok_far)
    scaled = (tokens * joined(ag_own, ag_far)).astype(BF16)
    mixer_gain = joined(mg_own, mg_far)
    square = jnp.sum(tokens * tokens, axis=1, keepdims=True)
    square_row = jnp.sum(jnp.where(diagonal, square, 0.0), axis=0, keepdims=True)
    for w, ref in enumerate((q1_w, q2_w)):
        part = jnp.dot(scaled, ref[...], preferred_element_type=F32)
        for t in range(2):
            qx[kv, 16 * w + 8 * t : 16 * w + 8 * t + 8, :] = part[:, 128 * t : 128 * t + 128]
    qx[kv, 32:33, :] = square_row
    for copy in kv_loads:
        copy.wait()
    for w, ref in enumerate((k1_w, k2_w)):
        part = jnp.dot(scaled, ref[...], preferred_element_type=F32)
        for t in range(2):
            rs[pl.ds(8 * t + w, 8, stride=16), :] = part[:, 128 * t : 128 * t + 128]
    part = jnp.dot(scaled, vw_w[...], preferred_element_type=F32)
    for t in range(HEADS):
        rs[pl.ds(8 * (t // 2) + 2 + t % 2, 8, stride=16), :] = part[:, 128 * t : 128 * t + 128]
    @pl.when(tp == 1)
    def _():
        pl.semaphore_wait(barrier, 2 * KV - 1)
        pl.semaphore_signal(ready.at[1], 1, device_id=partner, device_id_type=MESH)

    @pl.when(tp == 0)
    def _():
        pl.semaphore_wait(ready.at[1], 1)

    spread(0, lambda p: qx.at[kv], qx.at[kv])
    rx[kv] = rs[pl.ds(pl.multiple_of(8 * kv, 8), 8), :]

    wide = (256, 256)
    unit[...] = (lax.broadcasted_iota(jnp.int32, wide, 0) == lax.broadcasted_iota(jnp.int32, wide, 1)).astype(BF16)
    cache_loads[0].wait()

    def turn(c, carry):
        at = pl.multiple_of(c * 512, 512)
        for b in range(0, ROWS, 2):
            keys = jnp.concatenate([kc[b, pl.ds(at, 512), :], kc[b + 1, pl.ds(at, 512), :]], axis=1)
            turned = lax.dot_general(unit[...], keys, (((1,), (1,)), ((), ())), preferred_element_type=F32)
            kt[b // 2, :, pl.ds(at, 512)] = turned.astype(BF16)
        return carry

    lax.fori_loop(0, KEYS // 1024, turn, 0)
    spread(1, lambda p: rs.at[pl.ds(pl.multiple_of(8 * p, 8), 4), :], rx.at[kv, 0:4])
    lax.fori_loop(KEYS // 1024, KEYS // 512, turn, 0)
    cache_loads[1].wait()
    everything(0, qx.at[0 : KV - 1])

    def ratio_of(total):
        return lax.rsqrt(total / D + NORM_EPSILON)

    square_total = qx[0, 32:33, :]
    for s in range(1, KV):
        square_total = square_total + qx[s, 32:33, :]
    ratio_row = ratio_of(square_total)
    ratio = jnp.sum(jnp.where(diagonal, ratio_row, 0.0), axis=1, keepdims=True)
    cosine, sine = tab[0:1, :], tab[1:2, :]
    lead = lax.rem(lane, DH) < DH // 2

    def rotated(x):
        turned = jnp.where(lead, pltpu.roll(x, 128 - DH // 2, 1), pltpu.roll(x, DH // 2, 1))
        return (x * cosine + turned * sine).astype(BF16).astype(F32)

    def total_of(ref, at):
        total = ref[0, at : at + 8, :]
        for s in range(1, KV):
            total = total + ref[s, at : at + 8, :]
        return total

    query = [[rotated(total_of(qx, 16 * m + 8 * t) * ratio) for t in range(2)] for m in range(2)]
    low = lane < DH
    for h in range(HEADS):
        for m in range(2):
            x = query[m][h // 2]
            if h % 2 != m:
                x = pltpu.roll(x, DH, 1)
            qs[pl.ds(2 * h + m, 8, stride=8), :] = jnp.where(low if m == 0 else ~low, x, 0.0)

    key_head = lax.rem(lax.broadcasted_iota(jnp.int32, (16, 128), 1), HEADS)
    row_head = lax.rem(lax.broadcasted_iota(jnp.int32, (16, 128), 0), 8) // 2
    own_head = key_head == row_head
    scale = DH ** (-0.5)
    zero = jnp.zeros((8, 128), F32)
    step = 1024

    order = [lax.rem(across + 1 + t, 4) for t in range(ROWS // 2)]
    slot = 64 * (2 * lax.rem(kv, 8) + kv // 8)

    def score(t):
        rows = qs[pl.ds(pl.multiple_of(16 * order[t], 16), 16), :]
        left = jnp.concatenate(
            [
                jnp.concatenate([rows[0:8], zero], axis=1),
                jnp.concatenate([zero, rows[8:16]], axis=1),
            ],
            axis=0,
        ).astype(BF16)
        peak = jnp.full((16, 128), FLOOR, F32)
        for c in range(0, KEYS, step):
            s = jnp.dot(left, kt[order[t], :, c : c + step], preferred_element_type=F32)
            for i in range(0, step, 128):
                one = jnp.where(own_head, s[:, i : i + 128], FLOOR)
                peak = jnp.maximum(peak, one)
                sc[t % 2, :, c + i : c + i + 128] = one
        return jnp.max(peak, axis=1, keepdims=True)

    def new_token():
        everything(1, rx.at[0 : KV - 1, 0:4])
        row, share = kv // 2, lax.rem(kv, 2)
        new = total_of(rx, 0) * jnp.sum(jnp.where(sub[:, :1] == row, ratio, 0.0), axis=0, keepdims=True)
        asked = [
            jnp.sum(
                jnp.where(sub == row, jnp.where(share == 0, query[m][0], query[m][1]), 0.0), axis=0, keepdims=True
            )
            for m in range(2)
        ]
        product = jnp.where(sub == 0, asked[0], asked[1]) * rotated(new)
        wide_row = lax.broadcasted_iota(jnp.int32, (16, 128), 0)
        score_column = jnp.full((16, 1), FLOOR, F32)
        for k in range(2):
            half = jnp.sum(jnp.where(low if k == 0 else ~low, product, 0.0), axis=1, keepdims=True)
            for m in range(2):
                here = wide_row[:, :1] == 4 * along + 2 * k + m
                score_column = jnp.where(here, half[m : m + 1], score_column)
        new = new.astype(BF16).astype(F32)
        return score_column, jnp.where(lax.rem(wide_row, 4) < 2, new[2:3], new[3:4])

    stat = zero
    running = score(0)
    for t in range(ROWS // 2):
        b = 2 * order[t]
        peak = running
        if t + 1 < ROWS // 2:
            running = score(t + 1)
        else:
            own_score, own_value = new_token()
            peak = jnp.maximum(peak, own_score)
        total = jnp.zeros((16, 128), F32)
        weights = []
        for i in range(0, KEYS, 128):
            e = jnp.exp2((sc[t % 2, :, i : i + 128] - peak) * (scale * LOG2E))
            total = total + e
            weights.append(e.astype(BF16))
        total = jnp.sum(total, axis=1, keepdims=True)
        if t + 1 == ROWS // 2:
            own_weight = jnp.exp2((own_score - peak) * (scale * LOG2E))
            total = total + own_weight
        for k in range(2):
            at = 8 * (b + k)
            stat = jnp.where(lane - at == sub, peak[8 * k : 8 * k + 8] * scale, stat)
            stat = jnp.where(lane - 64 - at == sub, total[8 * k : 8 * k + 8], stat)
        if t + 1 == ROWS // 2:
            sx[pl.ds(kv, 1), :] = jnp.sum(stat, axis=0, keepdims=True)
            spread(2, lambda p: sx.at[pl.ds(kv, 1), :], sx.at[pl.ds(kv, 1), :])
        acc = jnp.zeros((16, 256), F32)
        for c in range(0, KEYS, step):
            values = jnp.concatenate([vc[b, c : c + step, :], vc[b + 1, c : c + step, :]], axis=1)
            w = jnp.concatenate(weights[c // 128 : (c + step) // 128], axis=1)
            acc = acc + jnp.dot(w, values, preferred_element_type=F32)
        acc = jnp.concatenate([acc[0:8, 0:128], acc[8:16, 128:256]], axis=0)
        if t + 1 == ROWS // 2:
            acc = acc + own_weight * own_value
        place = pl.ds(pl.multiple_of(slot + 16 * order[t], 16), 16)
        cx[place, :] = acc.astype(BF16)
        spread(3, lambda p: cx.at[place, :], cx.at[place, :])

    for copy in late_loads[:3]:
        copy.wait()
    second = jnp.zeros((8, 1), F32)
    for h in range(HEADS):
        second = jnp.where(sub[:, :1] == 2 * h, hsw[0:1, h : h + 1], second)
    gain = hg[...] * HEAD_SCALE
    square_mask = lax.rem(lax.broadcasted_iota(jnp.int32, (64, 128), 1), 64) == lax.broadcasted_iota(
        jnp.int32, (64, 128), 0
    )

    everything(2, sx.at[0 : KV - 1, :])
    stats = sx[...]
    factors = jnp.exp(stats - jnp.max(stats, axis=0, keepdims=True))
    weight_sum = jnp.sum(factors * pltpu.roll(stats, 64, 1), axis=0, keepdims=True)
    factors = factors * (1.0 / weight_sum)
    factors = jnp.where(low, factors[0:8], pltpu.roll(factors[8:16], DH, 1))
    high = factors.astype(BF16).astype(F32)
    mixing = jnp.concatenate(
        [
            jnp.concatenate(
                [jnp.where(square_mask, part[j : j + 1], 0.0).astype(BF16) for j in range(KV // 2)], axis=1
            )
            for part in (high, factors - high)
        ],
        axis=0,
    )
    everything(3, cx.at[0 : 64 * (KV - 1), :])
    both = jnp.dot(mixing, cx[...], preferred_element_type=F32)
    averaged = both[0:64] + both[64:128]
    for b in range(ROWS):
        one = averaged[8 * b : 8 * b + 8]
        difference = one - second * pltpu.roll(one, 7, 0)
        norm = lax.rsqrt(jnp.mean(difference * difference, axis=1, keepdims=True) + HEAD_EPSILON)
        df[8 * b : 8 * b + 8, :] = difference * norm * gain
    attended = jnp.concatenate([df[pl.ds(2 * h, 8, stride=8), :].astype(BF16) for h in range(HEADS)], axis=1)
    os_own[...] = jnp.dot(attended, ow_w[...], preferred_element_type=F32).astype(BF16)
    swap = pair(3, os_own, os_far)
    for copy in late_loads[3:]:
        copy.wait()
    swap.wait_recv()
    mixed = (tokens + (os_own[...].astype(F32) + os_far[...].astype(F32))).astype(BF16).astype(F32)
    mixer_scaled = (mixed * mixer_gain).astype(BF16)
    square = jnp.broadcast_to(jnp.sum(mixed * mixed, axis=1, keepdims=True), (8, 128))
    for w, ref in enumerate((gw_w, uw_w)):
        part = jnp.dot(mixer_scaled, ref[...], preferred_element_type=F32)
        for t in range(FT):
            row = (t // HT) * GR + w * HT + t % HT
            gs[pl.ds(row, 8, stride=2 * GR), :] = part[:, 128 * t : 128 * t + 128]
    high = square.astype(BF16).astype(F32)
    for half in range(2):
        gs[pl.ds(half * GR + 2 * HT, 8, stride=2 * GR), :] = high
        gs[pl.ds(half * GR + 2 * HT + 1, 8, stride=2 * GR), :] = square - high
    for j in range(KV):
        gb[j] = gs[j * GR : j * GR + GR, :].astype(BF16)
    gx[kv] = gb[kv]
    spread(5, lambda p: gb.at[p], gx.at[kv])
    everything(5, gx.at[0 : KV - 1])
    total = gx[0].astype(F32)
    for s in range(1, KV):
        total = total + gx[s].astype(F32)
    mixer_ratio = ratio_of(total[2 * HT : 2 * HT + 1] + total[2 * HT + 1 : 2 * HT + 2])
    gate = total[:HT] * mixer_ratio
    up = total[HT : 2 * HT] * mixer_ratio
    hidden = gate / (1.0 + jnp.exp(-gate)) * up
    mine = hx.at[KV * tp + kv, 0 : HT + 1]
    hx[KV * tp + kv, 0 : HT + 1, :] = jnp.concatenate([hidden, zero[0:1]], axis=0).astype(BF16)

    def share(p, core):
        pltpu.make_async_remote_copy(
            mine, mine, all_send.at[6], all_recv.at[6], device_id=(dp, p, core), device_id_type=MESH
        ).start()

    for p in peers:
        share(p, 1 - tp)
        share(p, tp)
    share(kv, 1 - tp)
    swap_down.wait_recv()
    everything(6, hx.at[0 : 2 * KV - 1, 0 : HT + 1])
    for s in range(2 * KV):
        hs[16 * s : 16 * s + 16, :] = hx[s].astype(F32)
    result = zero
    for core, weights in ((tp, dw_w), (1 - tp, dw_far)):
        at = pl.multiple_of(16 * KV * core, 8)
        hidden = jnp.concatenate(
            [
                jnp.concatenate([hs[pl.ds(at + 128 * k + t, 8, stride=16), :] for k in range(2)], axis=0).astype(BF16)
                for t in range(HT)
            ],
            axis=1,
        )
        down = jnp.concatenate([weights[0 : FF // 2, :], weights[FF // 2 : FF, :]], axis=1)
        part = jnp.dot(hidden, down, preferred_element_type=F32)
        ds[0:16, :] = part[:, 0:128]
        ds[16:32, :] = part[:, 128:256]
        part = ds[pl.ds(0, 8, stride=2), :] + ds[pl.ds(17, 8, stride=2), :]
        result = result + part.astype(BF16).astype(F32)
    result = mixed + result
    result = jnp.where(tp == 0, result, pltpu.roll(result, DH, 1))
    out_ref[...] = result[:, :64].astype(BF16)
    for copy in sends + spreads:
        copy.wait_send()


def shards(
    tokens, attention_gain, query_one, query_two, key_one, key_two, value_weight, head_second_weight, head_gain,
    out_weight, mixer_gain, gate_weight, up_weight, down_weight, key_cache, value_cache,
):
    any_space = pl.BlockSpec(memory_space=pl.ANY)
    vmem = pltpu.VMEM
    dma = pltpu.SemaphoreType.DMA
    return pl.pallas_call(
        layer_kernel,
        out_shape=pltpu.VMEM((ROWS, 64), BF16),
        in_specs=[any_space] * 17,
        out_specs=pl.BlockSpec(memory_space=pltpu.VMEM),
        scratch_shapes=[
            vmem((ROWS, 64), BF16), vmem((ROWS, 64), BF16),
            vmem((1, 64), BF16), vmem((1, 64), BF16), vmem((1, 64), BF16), vmem((1, 64), BF16),
            vmem((128, 256), BF16), vmem((128, 256), BF16), vmem((128, 256), BF16), vmem((128, 256), BF16),
            vmem((128, 512), BF16), vmem((1, HEADS), F32), vmem((1, 128), F32), vmem((512, 128), BF16),
            vmem((128, FF), BF16), vmem((128, FF), BF16), vmem((FF, 128), BF16),
            vmem((ROWS, KEYS, 128), BF16), vmem((ROWS, KEYS, 128), BF16), vmem((8, 128), F32),
            vmem((256, 256), BF16), vmem((ROWS // 2, 256, KEYS), BF16),
            vmem((KV, QR, 128), F32), vmem((KV * 8, 128), F32), vmem((KV, 8, 128), F32),
            vmem((KV * 64, 128), BF16), vmem((KV, 128), F32),
            vmem((KV * GR, 128), F32), vmem((KV, GR, 128), BF16), vmem((KV, GR, 128), BF16),
            vmem((2 * KV, 16, 128), BF16), vmem((2 * KV * 16, 128), F32), vmem((64, 128), F32),
            vmem((2, 16, KEYS), F32), vmem((64, 128), F32),
            vmem((8, 128), BF16), vmem((8, 128), BF16), vmem((FF, 128), BF16), vmem((32, 128), F32),
            pltpu.SemaphoreType.REGULAR((2,)), dma((17,)), dma((5,)), dma((5,)), dma((7,)), dma((7,)),
        ],
        compiler_params=pltpu.CompilerParams(
            collective_id=0, has_side_effects=True, vmem_limit_bytes=60 * 1024 * 1024
        ),
        name="layer",
    )(
        tokens, attention_gain.reshape(1, -1), query_one, query_two, key_one, key_two, value_weight,
        head_second_weight.reshape(1, -1), head_gain.reshape(1, -1), out_weight, mixer_gain.reshape(1, -1),
        gate_weight, up_weight, down_weight,
        key_cache.reshape(ROWS, KEYS, 128), value_cache.reshape(ROWS, KEYS, 128), jnp.asarray(rotary_tables()),
    )


def solution(mesh):
    both = ("kv", "tp")
    return jax.shard_map(
        shards,
        mesh=mesh,
        in_specs=(
            P("dp", both), P(both), P("kv", "tp"), P("kv", "tp"), P("kv", "tp"), P("kv", "tp"), P("kv", "tp"),
            P("tp"), P(), P("tp", "kv"), P(both), P("kv", "tp"), P("kv", "tp"), P("tp", "kv"),
            P("dp", "kv", "tp", None), P("dp", "kv", "tp", None),
        ),
        out_specs=P("dp", both),
        check_vma=False,
    )
```
